32 devices in a mesh: grp: 2 (over y), sp: 4 (over z), dp: 4 (over x, core).
Axes of the slice: x: 2, y: 2, z: 4, core: 2. Of those that a mesh axis runs over, the one named last changes fastest.
Arguments:
- tokens: bfloat16 [8, 512, 2048], P(('grp', 'dp'), 'sp'), parts along dimension 0, may hold values from -6 to 6
- forget_offset: float32 [8, 512], P(('grp', 'dp'), 'sp'), parts along dimension 0, may hold values from -1.2 to 1.2, as said below
- q_weight: bfloat16 [2048, 2048], P(None, 'dp'), may hold values from -0.125 to 0.125
- k_weight: bfloat16 [2048, 512], P(None, 'dp'), may hold values from -0.125 to 0.125
- v_weight: bfloat16 [2048, 512], P(None, 'dp'), may hold values from -0.125 to 0.125
- forget_weight: bfloat16 [2048, 16], replicated, may hold values from -0.125 to 0.125
- forget_bias: float32 [16], replicated, may hold values from 3 to 12
- score_gain: float32 [16], replicated, may hold values from 0.5 to 80
- out_gain: float32 [2048], replicated, may hold values from 0.1 to 1.9
Outputs:
- attended: bfloat16 [8, 512, 2048], P(('grp', 'dp'), 'sp'), parts along dimension 0
The draws below stay inside these ranges and needn't reach their ends.
There are 2 independent parts, one for each index of `grp`. The reference program is written for one: setup_inputs(seed, part) draws one part's arguments, and reference() takes and returns one part's arrays. A program takes and returns all parts, laid end to end along the dimension named above; an argument that names none is the same for every part. Nothing has to cross between parts.
Inputs may be any that keep to these rules, and one draw needn't show every extreme that they name: `forget_offset`: constant over aligned spans of 64 positions.
All inputs are finite; a program needn't handle non-finite values.
Results may differ from the reference program's by a relative error of at most 0.0085.
The reference program's roundings to bfloat16 on the way count: a program that leaves them out, or rounds other values in their place, can miss the bound.
Values may be sent and summed in bfloat16 or wider, within the bound.
A program may use at most 128 MiB of HBM per device.

```python
import jax
import jax.numpy as jnp
from jax import lax

WIDTH = 2048
HEADS = 16
KV_HEADS = 4
HEAD_DIM = 128
SEQ_LEN = 512
SEQS = 4


def draw_forget_offset(key, part):
    spans = (SEQ_LEN + 63) // 64
    levels = jax.random.uniform(key, (SEQS, spans), jnp.float32, -1.2, 1.2)
    return jnp.repeat(levels, 64, axis=1)[:, :SEQ_LEN]


def draw_forget_bias(key, part):
    head_order = jax.random.permutation(jax.random.fold_in(key, 11), HEADS)
    jitter = jax.random.uniform(jax.random.fold_in(key, 12), (HEADS,), jnp.float32, -0.3, 0.3)
    slow_level = jnp.log(2.0 * SEQ_LEN)
    fast_level = jnp.log(40.0)
    return jnp.where(head_order < HEADS // 2, slow_level, fast_level) + jitter


def draw_score_gain(key, part):
    return jnp.exp(jax.random.uniform(jax.random.fold_in(key, 22), (HEADS,), jnp.float32, jnp.log(0.7), jnp.log(2.5)))


def steps_of(stream_key, shape, cuts, smallest, largest):
    def one(position, parts):
        draws = jax.random.uniform(jax.random.fold_in(jax.random.fold_in(stream_key, 6), position), (parts,), jnp.float32, smallest / len(cuts), largest / len(cuts))
        return jnp.repeat(jnp.exp(draws), shape[position] // parts).reshape((-1,) + (1,) * (len(shape) - position - 1))

    loudness = one(*cuts[0])
    for cut in cuts[1:]:
        loudness = loudness * one(*cut)
    return loudness


def centred(own_key, shape, scale, bound, split=(), kind=jnp.bfloat16):
    array = scale * jax.random.normal(own_key, shape, jnp.float32)
    if split:
        array = array * steps_of(own_key, shape, split, -0.22, 0.18)
    return jnp.clip(array, -bound, bound).astype(kind)


def setup_inputs(seed: int = 0, part: int = 0) -> dict:
    key_of = jax.random.split(jax.random.key(seed), 10)
    part_splits = jax.random.split(jax.random.fold_in(key_of[9], part), 10)
    return {
        "tokens": centred(part_splits[0], (SEQS, SEQ_LEN, WIDTH), 1.0, 6.0, ((0, 4), (1, 4))),
        "forget_offset": draw_forget_offset(jax.random.fold_in(jax.random.fold_in(key_of[9], part), 71), part),
        "q_weight": centred(key_of[2], (WIDTH, HEADS * HEAD_DIM), WIDTH ** -0.5, 0.125, ((1, 4),)),
        "k_weight": centred(key_of[3], (WIDTH, KV_HEADS * HEAD_DIM), WIDTH ** -0.5, 0.125, ((1, 4),)),
        "v_weight": centred(key_of[4], (WIDTH, KV_HEADS * HEAD_DIM), WIDTH ** -0.5, 0.125, ((1, 4),)),
        "forget_weight": centred(key_of[5], (WIDTH, HEADS), WIDTH ** -0.5, 0.125),
        "forget_bias": draw_forget_bias(jax.random.fold_in(key_of[9], 71), part),
        "score_gain": draw_score_gain(jax.random.fold_in(key_of[9], 71), part),
        "out_gain": jnp.clip(1.0 + 0.18 * jax.random.normal(key_of[8], (HEADS * HEAD_DIM,), jnp.float32), 0.1, 1.9),
    }


NEG = -1e+30
QK_FLOOR = 0.1
OUT_FLOOR = 0.001

def head_norm(vectors, floor):
    return vectors * lax.rsqrt(lax.optimization_barrier(jnp.mean(vectors * vectors, axis=-1, keepdims=True)) + floor)

def attend_sequence(token_rows, offset_rows, q_weight, k_weight, v_weight, forget_weight, forget_bias, score_gain, out_gain):
    length = token_rows.shape[0]
    head_count = forget_bias.shape[0]
    head_dim = out_gain.shape[0] // head_count
    kv_heads = k_weight.shape[1] // head_dim
    group_size = head_count // kv_heads
    queries = jnp.dot(token_rows, q_weight, preferred_element_type=jnp.float32).astype(jnp.bfloat16)
    keys_proj = jnp.dot(token_rows, k_weight, preferred_element_type=jnp.float32).astype(jnp.bfloat16)
    values_proj = jnp.dot(token_rows, v_weight, preferred_element_type=jnp.float32).astype(jnp.bfloat16)
    forget_input = (jnp.dot(token_rows, forget_weight, preferred_element_type=jnp.float32) + offset_rows[:, None]).astype(jnp.bfloat16)
    log_gate = jax.nn.log_sigmoid(forget_input.astype(jnp.float32) + forget_bias[None, :])
    cumulative = jnp.cumsum(log_gate, axis=0).reshape(length, kv_heads, group_size)
    query_unit = head_norm(queries.astype(jnp.float32).reshape(length, kv_heads, group_size, head_dim), QK_FLOOR).astype(jnp.bfloat16)
    key_unit = head_norm(keys_proj.astype(jnp.float32).reshape(length, kv_heads, head_dim), QK_FLOOR).astype(jnp.bfloat16)
    value_heads = values_proj.reshape(length, kv_heads, head_dim)
    factor = (score_gain * head_dim ** (-0.5)).reshape(kv_heads, group_size)
    out_gains = out_gain.reshape(kv_heads, group_size, head_dim)
    span_rows = 512 if length % 512 == 0 else length
    positions = jnp.arange(length, dtype=jnp.int32)
    key_totals = jnp.transpose(cumulative, (1, 2, 0))

    def one_block(block_index):
        first = (block_index * span_rows).astype(jnp.int32)
        query_block = lax.dynamic_slice_in_dim(query_unit, first, span_rows, 0)
        query_totals = lax.dynamic_slice_in_dim(cumulative, first, span_rows, 0)
        scores = jnp.einsum('qkgd,skd->kgqs', query_block.astype(jnp.float32), key_unit.astype(jnp.float32))
        scores = scores * factor[:, :, None, None] + jnp.transpose(query_totals, (1, 2, 0))[..., None] - key_totals[:, :, None, :]
        allowed = positions[None, :] <= (first + jnp.arange(span_rows, dtype=jnp.int32))[:, None]
        scores = jnp.where(allowed[None, None], scores, NEG)
        row_peak = lax.optimization_barrier(jnp.max(scores, axis=-1, keepdims=True))
        exponent = jnp.exp(scores - row_peak)
        weights = (exponent / lax.optimization_barrier(jnp.sum(exponent, axis=-1, keepdims=True))).astype(jnp.bfloat16)
        mixed = jnp.einsum('kgqs,skd->qkgd', weights.astype(jnp.float32), value_heads.astype(jnp.float32))
        return (head_norm(mixed, OUT_FLOOR) * out_gains).astype(jnp.bfloat16)
    outputs = lax.map(one_block, jnp.arange(length // span_rows, dtype=jnp.int32))
    return outputs.reshape(length, head_count * head_dim)

def reference(tokens, forget_offset, q_weight, k_weight, v_weight, forget_weight, forget_bias, score_gain, out_gain):

    def attend_one(one_pair):
        return attend_sequence(one_pair[0], one_pair[1], q_weight, k_weight, v_weight, forget_weight, forget_bias, score_gain, out_gain)
    return lax.map(attend_one, (tokens, forget_offset))
```

```python
import functools

import jax
import jax.numpy as jnp
from jax import lax
from jax.experimental import pallas as pl
from jax.experimental.pallas import tpu as pltpu
from jax.sharding import PartitionSpec as P

NEG = -1e30
QK_FLOOR = 0.1
OUT_FLOOR = 0.001


def head_norm(vectors, floor):
    return vectors * lax.rsqrt(jnp.mean(vectors * vectors, axis=-1, keepdims=True) + floor)


def heads_on_sp(
    tokens,
    forget_offset,
    q_weight,
    k_weight,
    v_weight,
    forget_weight,
    forget_bias,
    score_gain,
    out_gain,
):
    own_rows = tokens[0]
    tok_count = own_rows.shape[0]
    head_count = forget_bias.shape[0]
    head_dim = out_gain.shape[0] // head_count
    kv_heads = k_weight.shape[1] * lax.axis_size("dp") // head_dim
    spread = lax.axis_size("sp")
    local_heads = head_count // spread
    local_kv = max(1, kv_heads // spread)
    group_size = local_heads // local_kv
    everyone = lax.all_gather(tokens, "dp", axis=0, tiled=True)
    seq_count = everyone.shape[0]
    flat_rows = everyone.reshape(seq_count * tok_count, everyone.shape[2])
    query_cols = (
        jnp.dot(flat_rows, q_weight, preferred_element_type=jnp.float32)
        .astype(jnp.bfloat16)
        .reshape(seq_count, tok_count, -1)
    )
    key_cols = (
        jnp.dot(flat_rows, k_weight, preferred_element_type=jnp.float32)
        .astype(jnp.bfloat16)
        .reshape(seq_count, tok_count, -1)
    )
    value_cols = (
        jnp.dot(flat_rows, v_weight, preferred_element_type=jnp.float32)
        .astype(jnp.bfloat16)
        .reshape(seq_count, tok_count, -1)
    )
    query_mine, key_mine, value_mine = (
        lax.all_to_all(query_cols, "dp", split_axis=0, concat_axis=2, tiled=True),
        lax.all_to_all(key_cols, "dp", split_axis=0, concat_axis=2, tiled=True),
        lax.all_to_all(value_cols, "dp", split_axis=0, concat_axis=2, tiled=True),
    )
    queries = query_mine[0]
    keys_proj = key_mine[0]
    values_proj = value_mine[0]
    forget_input = (
        jnp.dot(own_rows, forget_weight, preferred_element_type=jnp.float32)
        + forget_offset[0][:, None]
    ).astype(jnp.bfloat16)
    query_send = queries.reshape(tok_count, spread, local_heads, head_dim)
    forget_send = forget_input.reshape(tok_count, spread, local_heads)
    if kv_heads >= spread:
        key_send = keys_proj.reshape(tok_count, spread, local_kv, head_dim)
        value_send = values_proj.reshape(tok_count, spread, local_kv, head_dim)
    else:
        copies = spread // kv_heads
        key_send = jnp.broadcast_to(
            keys_proj.reshape(tok_count, kv_heads, 1, head_dim),
            (tok_count, kv_heads, copies, head_dim),
        ).reshape(tok_count, spread, 1, head_dim)
        value_send = jnp.broadcast_to(
            values_proj.reshape(tok_count, kv_heads, 1, head_dim),
            (tok_count, kv_heads, copies, head_dim),
        ).reshape(tok_count, spread, 1, head_dim)
    query_head, forget_head, key_head, value_head = (
        lax.all_to_all(query_send, "sp", split_axis=1, concat_axis=0, tiled=True),
        lax.all_to_all(forget_send, "sp", split_axis=1, concat_axis=0, tiled=True),
        lax.all_to_all(key_send, "sp", split_axis=1, concat_axis=0, tiled=True),
        lax.all_to_all(value_send, "sp", split_axis=1, concat_axis=0, tiled=True),
    )
    length = query_head.shape[0]
    first_head = lax.axis_index("sp") * local_heads
    bias_local = lax.dynamic_slice_in_dim(forget_bias, first_head, local_heads, 0)
    gain_local = lax.dynamic_slice_in_dim(score_gain, first_head, local_heads, 0)
    norm_local = lax.dynamic_slice_in_dim(
        out_gain, first_head * head_dim, local_heads * head_dim, 0
    )
    log_gate = jax.nn.log_sigmoid(
        forget_head.reshape(length, local_heads).astype(jnp.float32) + bias_local[None, :]
    )
    cumulative = jnp.cumsum(log_gate, axis=0).reshape(length, local_kv, group_size)
    query_unit = head_norm(query_head.astype(jnp.float32), QK_FLOOR).astype(jnp.bfloat16)
    key_unit = head_norm(
        key_head.reshape(length, local_kv, head_dim).astype(jnp.float32), QK_FLOOR
    ).astype(jnp.bfloat16)
    value_heads = value_head.reshape(length, local_kv, head_dim)
    factor = (gain_local * head_dim ** (-0.5)).reshape(local_kv, group_size)
    out_gains = norm_local.reshape(local_kv, group_size, head_dim)
    key_totals = jnp.transpose(cumulative, (1, 2, 0))
    span_rows = 512
    positions = jnp.arange(length, dtype=jnp.int32)

    def attend_block(block_index):
        first = block_index * span_rows
        query_block = lax.dynamic_slice_in_dim(query_unit, first, span_rows, 0)
        query_totals = lax.dynamic_slice_in_dim(cumulative, first, span_rows, 0)
        scores = jnp.einsum(
            "qkgd,skd->kgqs", query_block, key_unit, preferred_element_type=jnp.float32
        )
        scores = (
            scores * factor[:, :, None, None]
            + jnp.transpose(query_totals, (1, 2, 0))[..., None]
            - key_totals[:, :, None, :]
        )
        allowed = positions[None, :] <= (first + jnp.arange(span_rows, dtype=jnp.int32))[:, None]
        scores = jnp.where(allowed[None, None], scores, NEG)
        row_peak = jnp.max(scores, axis=-1, keepdims=True)
        exponent = jnp.exp(scores - row_peak)
        weights = (exponent / jnp.sum(exponent, axis=-1, keepdims=True)).astype(jnp.bfloat16)
        mixed = jnp.einsum(
            "kgqs,skd->qkgd", weights, value_heads, preferred_element_type=jnp.float32
        )
        return (head_norm(mixed, OUT_FLOOR) * out_gains).astype(jnp.bfloat16)

    outputs = lax.map(attend_block, jnp.arange(length // span_rows, dtype=jnp.int32))
    outputs = outputs.reshape(length, local_heads, head_dim)
    back_rows = lax.all_to_all(outputs, "sp", split_axis=0, concat_axis=1, tiled=True)
    return back_rows.reshape(1, tok_count, head_count * head_dim)


def heads_on_dp(
    tokens,
    forget_offset,
    q_weight,
    k_weight,
    v_weight,
    forget_weight,
    forget_bias,
    score_gain,
    out_gain,
):
    tok_count = tokens.shape[1]
    head_count = forget_bias.shape[0]
    head_dim = out_gain.shape[0] // head_count
    seq_count = lax.axis_size("dp")
    kv = k_weight.shape[1] // head_dim
    heads = q_weight.shape[1] // head_dim
    group = heads // kv
    everyone = lax.all_gather(tokens, "dp", axis=0, tiled=True)
    offsets = lax.all_gather(forget_offset, "dp", axis=0, tiled=True)
    flat = everyone.reshape(seq_count * tok_count, -1)
    first = lax.axis_index("dp") * heads

    def mine(array):
        return lax.dynamic_slice_in_dim(array, first, heads, array.ndim - 1)

    def project(weight):
        return jnp.dot(flat, weight, preferred_element_type=jnp.float32).astype(jnp.bfloat16)

    key_unit = head_norm(
        project(k_weight).astype(jnp.float32).reshape(seq_count, tok_count, kv, head_dim), QK_FLOOR
    ).astype(jnp.bfloat16)
    values = project(v_weight).reshape(seq_count, tok_count, kv, head_dim)
    pair = lax.all_gather(jnp.stack([key_unit, values]), "sp", axis=2, tiled=True)
    forget_input = (
        jnp.dot(flat, mine(forget_weight), preferred_element_type=jnp.float32)
        + offsets.reshape(-1)[:, None]
    ).astype(jnp.bfloat16)
    log_gate = jax.nn.log_sigmoid(forget_input.astype(jnp.float32) + mine(forget_bias)[None, :])
    gates = lax.all_gather(
        log_gate.reshape(seq_count, tok_count, heads), "sp", axis=1, tiled=True
    )
    cumulative = jnp.cumsum(gates, axis=1)
    length = gates.shape[1]
    start = lax.axis_index("sp") * tok_count
    own = lax.dynamic_slice_in_dim(cumulative, start, tok_count, 1)
    query_unit = head_norm(
        project(q_weight).astype(jnp.float32).reshape(seq_count, tok_count, kv, group, head_dim),
        QK_FLOOR,
    ).astype(jnp.bfloat16)
    factor = (mine(score_gain) * head_dim ** (-0.5)).reshape(kv, group)
    scores = jnp.einsum(
        "bqkgd,bskd->bkgqs", query_unit, pair[0], preferred_element_type=jnp.float32
    )
    by_head = jnp.transpose(own.reshape(seq_count, tok_count, kv, group), (0, 2, 3, 1))
    by_key = jnp.transpose(cumulative.reshape(seq_count, length, kv, group), (0, 2, 3, 1))
    scores = (
        scores * factor[None, :, :, None, None] + by_head[..., None] - by_key[..., None, :]
    )
    allowed = jnp.arange(length)[None, :] <= (start + jnp.arange(tok_count))[:, None]
    scores = jnp.where(allowed, scores, NEG)
    exponent = jnp.exp(scores - jnp.max(scores, axis=-1, keepdims=True))
    weights = (exponent / jnp.sum(exponent, axis=-1, keepdims=True)).astype(jnp.bfloat16)
    mixed = jnp.einsum(
        "bkgqs,bskd->bqkgd", weights, pair[1], preferred_element_type=jnp.float32
    )
    gains = lax.dynamic_slice_in_dim(out_gain, first * head_dim, heads * head_dim, 0)
    outputs = (head_norm(mixed, OUT_FLOOR) * gains.reshape(kv, group, head_dim)).astype(
        jnp.bfloat16
    )
    outputs = outputs.reshape(seq_count, tok_count, heads * head_dim)
    return lax.all_to_all(outputs, "dp", split_axis=0, concat_axis=2, tiled=True)


LOG2E = 1.4426950408889634


def fused_kernel(
    tok_in,
    off_in,
    qw_in,
    kw_in,
    vw_in,
    fw_in,
    bias_in,
    gain_in,
    norm_in,
    result,
    tok,
    qw,
    kvw,
    fw,
    off,
    bias_row,
    gain,
    norm,
    q_unit,
    kv,
    running_all,
    gates,
    sent,
    load_sem,
    off_send,
    off_recv,
    beside_send,
    beside_recv,
    over_send,
    over_recv,
    onward_send,
    onward_recv,
    gate_send,
    gate_recv,
    kv_send,
    kv_recv,
    back_send,
    out_send,
    out_recv,
):
    d = lax.axis_index("dp")
    s = lax.axis_index("sp")
    spread = lax.axis_size("sp")
    rows, width = tok_in.shape
    half = rows // 2
    cols = qw_in.shape[1]
    head_dim = kw_in.shape[1]
    heads = cols // head_dim
    seqs = tok.shape[0]
    chip, core = d // 2, d % 2
    last = spread - 1
    scope = jax.named_scope

    def peer(step):
        across = step // 2
        own_chip = (1 - across) * ((core + step % 2) % 2)
        return ((chip + across) % 2) * 2 + across * (step % 2) + own_chip

    def seen_as(step):
        return (step // 2) * (2 + core) + (1 - step // 2) * step

    def remote(src, dst, send, recv, **target):
        return pltpu.make_async_remote_copy(
            src_ref=src,
            dst_ref=dst,
            send_sem=send,
            recv_sem=recv,
            device_id=target,
            device_id_type=pl.DeviceIdType.MESH,
        )

    barrier = pltpu.get_barrier_semaphore()
    for step in range(1, seqs):
        pl.semaphore_signal(
            barrier, inc=1, device_id={"dp": peer(step)}, device_id_type=pl.DeviceIdType.MESH
        )
    for step in range(1, spread):
        pl.semaphore_signal(
            barrier,
            inc=1,
            device_id={"sp": (s + step) % spread},
            device_id_type=pl.DeviceIdType.MESH,
        )

    def load(src, dst, index):
        copy = pltpu.make_async_copy(src, dst, load_sem.at[index])
        copy.start()
        return copy

    load_tok = load(tok_in, tok.at[0], 0)
    load_off = load(off_in, off.at[0], 1)
    load_k = load(kw_in, kvw.at[:, pl.ds(0, head_dim)], 2)
    load_v = load(vw_in, kvw.at[:, pl.ds(head_dim, head_dim)], 3)
    load_f = load(fw_in, fw, 4)
    load_b = load(bias_in, bias_row, 5)
    load_g = load(gain_in, gain, 6)
    load_n = load(norm_in, norm, 7)
    load_q = load(qw_in, qw, 8)

    load_tok.wait()
    load_off.wait()
    with scope("bar"):
        pl.semaphore_wait(barrier, seqs - 1 + spread - 1)

    offs = [
        remote(off.at[0], off.at[seen_as(step)], off_send.at[0], off_recv.at[0], dp=peer(step))
        for step in range(1, seqs)
    ]
    for copy in offs:
        copy.start()

    def half_of(index):
        return pl.ds(pl.multiple_of(index * half, half), half)

    beside = [
        remote(
            tok.at[0, half_of(part)], tok.at[1, half_of(part)], beside_send.at[0],
            beside_recv.at[i], dp=peer(1),
        )
        for i, part in enumerate((1 - core, core))
    ]
    over = [
        remote(
            tok.at[held, half_of(core)], tok.at[2 + i, half_of(core)], over_send.at[0],
            over_recv.at[i], dp=(1 - chip) * 2 + core,
        )
        for i, held in enumerate((core, 1 - core))
    ]
    onward = [
        remote(
            tok.at[2 + i, half_of(core)], tok.at[2 + i, half_of(core)], onward_send.at[0],
            onward_recv.at[i], dp=peer(1),
        )
        for i in range(2)
    ]

    @pl.when(core == 0)
    def _():
        over[0].start()

    for copy in beside:
        copy.start()

    def unit(vectors):
        vectors = vectors.astype(jnp.bfloat16).astype(jnp.float32)
        return head_norm(vectors, QK_FLOOR).astype(jnp.bfloat16)

    pieces = [(0, 0, rows), (1, 0, rows), (2, 0, half), (2, half, half), (3, 0, half), (3, half, half)]

    def returned(slot):
        return slot < 2

    def to_each(act):
        for target in range(last, 0, -1):

            @pl.when(s < target)
            def _():
                act(target)

    def kv_copy(slot, first, count, target):
        piece = kv.at[slot, :, pl.ds(pl.multiple_of(s * rows + first, half), count)]
        return remote(piece, piece, kv_send.at[target], kv_recv.at[slot], sp=target)

    def gate_copy(slot, target):
        piece = gates.at[slot, s]
        return remote(piece, piece, gate_send.at[target], gate_recv.at[slot], sp=target)

    def back_copy(slot):
        piece = kv.at[slot, :, pl.ds(0, (last - 1) * rows)]
        return remote(piece, piece, back_send.at[0], kv_recv.at[slot], sp=last - 1)

    def send_kv(p):
        slot, first, count = pieces[p]

        def act(target):
            if not (target == last - 1 and returned(slot)):
                kv_copy(slot, first, count, target).start()

        to_each(act)

    def send_gate(slot):
        to_each(lambda target: gate_copy(slot, target).start())

    def project_kv(p):
        slot, first, count = pieces[p]
        pair = jnp.dot(
            tok[slot, first : first + count], kvw[...], preferred_element_type=jnp.float32
        )
        here = pl.ds(pl.multiple_of(s * rows + first, half), count)
        kv[slot, 0, here] = unit(pair[:, :head_dim])
        kv[slot, 1, here] = pair[:, head_dim:].astype(jnp.bfloat16)

    def project_q(slot):
        queries = jnp.dot(tok[slot], qw[...], preferred_element_type=jnp.float32)
        for h in range(heads):
            q_unit[slot, pl.ds(h * rows, rows)] = unit(
                queries[:, h * head_dim : (h + 1) * head_dim]
            )

    count = bias_in.shape[1]

    def gate(slot):
        forget_input = (
            lax.dot_general(
                fw[...], tok[slot], (((1,), (1,)), ((), ())), preferred_element_type=jnp.float32
            )
            + off[slot]
        ).astype(jnp.bfloat16)
        square = (count, count)
        diagonal = lax.broadcasted_iota(jnp.int32, square, 0) == lax.broadcasted_iota(
            jnp.int32, square, 1
        )
        bias = jnp.sum(
            jnp.where(diagonal, jnp.broadcast_to(bias_row[...], square), 0.0),
            axis=1,
            keepdims=True,
        )
        gate_arg = forget_input.astype(jnp.float32) + bias
        log_gate = jnp.minimum(gate_arg, 0.0) - jnp.log1p(jnp.exp(-jnp.abs(gate_arg)))
        before = lax.broadcasted_iota(jnp.int32, (rows, rows), 0)
        after = lax.broadcasted_iota(jnp.int32, (rows, rows), 1)
        upto = (before <= after).astype(jnp.bfloat16)
        high = log_gate.astype(jnp.bfloat16)
        rest = log_gate - high.astype(jnp.float32)
        middle = rest.astype(jnp.bfloat16)
        low = (rest - middle.astype(jnp.float32)).astype(jnp.bfloat16)
        running = (
            jnp.dot(low, upto, preferred_element_type=jnp.float32)
            + jnp.dot(middle, upto, preferred_element_type=jnp.float32)
            + jnp.dot(high, upto, preferred_element_type=jnp.float32)
        )
        running_all[...] = running * LOG2E
        own = running_all[pl.ds(d * heads, heads)]
        spare = gates.shape[2] - heads
        if spare:
            own = jnp.concatenate([own, jnp.zeros((spare, rows), jnp.float32)], axis=0)
        gates[slot, s] = own

    mine = pl.ds(pl.multiple_of(d * cols, cols), cols)

    def out_copy(slot):
        return remote(
            sent.at[slot], result.at[:, mine], out_send.at[0], out_recv.at[0], dp=peer(slot)
        )

    def attend(slot, blocks):
        span = blocks * rows
        later = jnp.zeros((gates.shape[2], 1), jnp.float32)
        totals = [gates[slot, blocks - 1]]
        for b in range(blocks - 2, -1, -1):
            local_sum = gates[slot, b]
            later = later + local_sum[:, rows - 1 :]
            totals.insert(0, local_sum - later)
        allowed = lax.broadcasted_iota(jnp.int32, (rows, rows), 1) <= lax.broadcasted_iota(
            jnp.int32, (rows, rows), 0
        )
        keys = kv[slot, 0, :span]
        values = kv[slot, 1, :span]
        each = range(heads)
        raw = [
            lax.dot_general(
                q_unit[slot, pl.ds(h * rows, rows)],
                keys,
                (((1,), (1,)), ((), ())),
                preferred_element_type=jnp.float32,
            )
            for h in each
        ]
        scores = []
        for h in each:
            factor = gain[0, d * heads + h] * (head_dim ** (-0.5) * LOG2E)
            parts = [
                raw[h][:, b * rows : (b + 1) * rows] * factor - totals[b][h : h + 1, :]
                for b in range(blocks)
            ]
            parts[-1] = jnp.where(allowed, parts[-1], NEG)
            scores.append(parts)
        peaks = [
            jnp.max(functools.reduce(jnp.maximum, parts), axis=-1, keepdims=True)
            for parts in scores
        ]
        exponents = [[jnp.exp2(part - peaks[h]) for part in scores[h]] for h in each]
        scales = [
            1.0 / jnp.sum(functools.reduce(jnp.add, parts), axis=-1, keepdims=True)
            for parts in exponents
        ]
        weights = [
            jnp.concatenate(
                [(part * scales[h]).astype(jnp.bfloat16) for part in exponents[h]], axis=1
            )
            for h in each
        ]
        mixed = [jnp.dot(weights[h], values, preferred_element_type=jnp.float32) for h in each]
        for h in each:
            place = pl.ds(pl.multiple_of(d * cols + h * head_dim, head_dim), head_dim)
            outcome = (head_norm(mixed[h], OUT_FLOOR) * norm[:, place]).astype(jnp.bfloat16)
            if slot == 0:
                result[:, place] = outcome
            else:
                sent[slot, :, h * head_dim : (h + 1) * head_dim] = outcome
        if slot > 0:
            out_copy(slot).start()

    def arrived(ref, semaphore):
        pltpu.make_async_copy(ref, ref, semaphore).wait()

    def await_kv(slot, k):
        if k > 0:
            with scope(f"wkv{slot}"):
                arrived(gates.at[slot, pl.ds(0, k)], gate_recv.at[slot])
                arrived(kv.at[slot, :, pl.ds(0, k * rows)], kv_recv.at[slot])

    def send_back(slot):
        @pl.when(s == last)
        def _():
            await_kv(slot, last)
            back_copy(slot).start()

    def attend_at(slot, places):
        for k in places:

            @pl.when(s == k)
            def _():
                if not (k == last and returned(slot)):
                    await_kv(slot, k)
                with scope(f"att{slot}"):
                    attend(slot, k + 1)

    def arrive(i, part):
        with scope(f"wx{i}{part}"):

            @pl.when(core == part)
            def _():
                over[i].wait_recv()
                onward[i].start()

            @pl.when(core != part)
            def _():
                onward[i].wait_recv()

    load_k.wait()
    load_v.wait()
    with scope("pkv0"):
        project_kv(0)
    send_kv(0)
    with scope("wb0"):
        beside[0].wait_recv()

    @pl.when(core == 1)
    def _():
        over[0].start()

    over[1].start()
    load_f.wait()
    load_b.wait()
    with scope("wb1"):
        beside[1].wait_recv()
    with scope("pkv1g0"):
        gate(0)
        project_kv(1)
    send_gate(0)
    send_kv(1)
    load_q.wait()
    load_g.wait()
    load_n.wait()
    with scope("woff"):
        arrived(off.at[pl.ds(1, seqs - 1)], off_recv.at[0])
    with scope("pq01g1"):
        gate(1)
        project_q(0)
        project_q(1)
    send_gate(1)
    arrive(0, 0)
    with scope("pkv2"):
        project_kv(2)
    send_kv(2)
    arrive(0, 1)
    with scope("pkv3g2"):
        gate(2)
        project_kv(3)
    send_gate(2)
    send_kv(3)
    with scope("pq2"):
        project_q(2)
    send_back(0)
    arrive(1, 0)
    with scope("pkv4"):
        project_kv(4)
    send_kv(4)
    send_back(1)
    everywhere = list(range(spread))
    most = [k for k in everywhere if k != last - 1]
    attend_at(0, most)
    arrive(1, 1)
    with scope("pkv5g3"):
        gate(3)
        project_kv(5)
    send_gate(3)
    send_kv(5)
    with scope("pq3"):
        project_q(3)
    attend_at(1, most)
    attend_at(2, everywhere)
    attend_at(0, [last - 1])
    attend_at(1, [last - 1])
    attend_at(3, everywhere)

    with scope("flush"):
        arrived(sent.at[pl.ds(1, seqs - 1)], out_recv.at[0])
    with scope("drain"):
        arrived(sent.at[pl.ds(1, seqs - 1)], out_send.at[0])
        arrived(off.at[pl.ds(1, seqs - 1)], off_send.at[0])
        for semaphore in (beside_send, over_send, onward_send):
            arrived(tok.at[0], semaphore.at[0])

        def sent_to(target):
            arrived(gates.at[pl.ds(0, seqs), 0], gate_send.at[target])
            skipped = sum(target == last - 1 and returned(slot) for slot in range(seqs))
            arrived(kv.at[pl.ds(skipped, seqs - skipped), :, pl.ds(0, rows)], kv_send.at[target])

        to_each(sent_to)

        @pl.when(s == last)
        def _():
            many = sum(returned(slot) for slot in range(seqs))
            arrived(kv.at[pl.ds(0, many), :, pl.ds(0, (last - 1) * rows)], back_send.at[0])


def fused(
    tokens,
    forget_offset,
    q_weight,
    k_weight,
    v_weight,
    forget_weight,
    forget_bias,
    score_gain,
    out_gain,
):
    rows, width = tokens.shape[1:]
    head_count = forget_bias.shape[0]
    head_dim = out_gain.shape[0] // head_count
    seqs = lax.axis_size("dp")
    spread = lax.axis_size("sp")
    cols = q_weight.shape[1]
    heads = cols // head_dim
    padded = -(-heads // 8) * 8
    outside = pl.BlockSpec(memory_space=pltpu.HBM)
    dma = pltpu.SemaphoreType.DMA
    out = pl.pallas_call(
        fused_kernel,
        out_shape=pltpu.VMEM((rows, seqs * cols), jnp.bfloat16),
        in_specs=[outside] * 9,
        out_specs=pl.BlockSpec(memory_space=pltpu.VMEM),
        scratch_shapes=[
            pltpu.VMEM((seqs, rows, width), jnp.bfloat16),
            pltpu.VMEM((width, cols), jnp.bfloat16),
            pltpu.VMEM((width, 2 * head_dim), jnp.bfloat16),
            pltpu.VMEM((head_count, width), jnp.bfloat16),
            pltpu.VMEM((seqs, 1, rows), jnp.float32),
            pltpu.VMEM((1, head_count), jnp.float32),
            pltpu.SMEM((1, head_count), jnp.float32),
            pltpu.VMEM((1, head_count * head_dim), jnp.float32),
            pltpu.VMEM((seqs, heads * rows, head_dim), jnp.bfloat16),
            pltpu.VMEM((seqs, 2, spread * rows, head_dim), jnp.bfloat16),
            pltpu.VMEM((head_count, rows), jnp.float32),
            pltpu.VMEM((seqs, spread, padded, rows), jnp.float32),
            pltpu.VMEM((seqs, rows, cols), jnp.bfloat16),
            dma((9,)),
            dma((1,)),
            dma((1,)),
            dma((1,)),
            dma((2,)),
            dma((1,)),
            dma((2,)),
            dma((1,)),
            dma((2,)),
            dma((spread,)),
            dma((seqs,)),
            dma((spread,)),
            dma((seqs,)),
            dma((1,)),
            dma((1,)),
            dma((1,)),
        ],
        compiler_params=pltpu.CompilerParams(
            collective_id=0, has_side_effects=True
        ),
    )(
        tokens[0],
        forget_offset,
        q_weight,
        k_weight,
        v_weight,
        forget_weight.T,
        forget_bias[None, :],
        score_gain[None, :],
        out_gain[None, :],
    )
    return out[None]


def local(*args):
    tokens, k_weight, forget_bias, out_gain = args[0], args[3], args[6], args[8]
    head_dim = out_gain.shape[0] // forget_bias.shape[0]
    fits = tokens.shape[0] == 1 and tokens.shape[1] % 128 == 0 and head_dim % 128 == 0
    if (
        lax.axis_size("dp") == 4
        and 2 < lax.axis_size("sp") <= 4
        and k_weight.shape[1] == head_dim
        and fits
    ):
        return fused(*args)
    if k_weight.shape[1] % head_dim == 0 and tokens.shape[0] == 1:
        return heads_on_dp(*args)
    return heads_on_sp(*args)


def solution(mesh):
    in_specs = (
        P(("grp", "dp"), "sp", None),
        P(("grp", "dp"), "sp"),
        P(None, "dp"),
        P(None, "dp"),
        P(None, "dp"),
        P(),
        P(),
        P(),
        P(),
    )
    out_specs = P(("grp", "dp"), "sp", None)
    return jax.shard_map(local, mesh=mesh, in_specs=in_specs, out_specs=out_specs, check_vma=False)
```

```python
import functools

import jax
import jax.numpy as jnp
from jax import lax
from jax.experimental import pallas as pl
from jax.experimental.pallas import tpu as pltpu
from jax.sharding import PartitionSpec as P

NEG = -1e30
QK_FLOOR = 0.1
OUT_FLOOR = 0.001


def head_norm(vectors, floor):
    return vectors * lax.rsqrt(jnp.mean(vectors * vectors, axis=-1, keepdims=True) + floor)


def heads_on_sp(
    tokens,
    forget_offset,
    q_weight,
    k_weight,
    v_weight,
    forget_weight,
    forget_bias,
    score_gain,
    out_gain,
):
    own_rows = tokens[0]
    tok_count = own_rows.shape[0]
    head_count = forget_bias.shape[0]
    head_dim = out_gain.shape[0] // head_count
    kv_heads = k_weight.shape[1] * lax.axis_size("dp") // head_dim
    spread = lax.axis_size("sp")
    local_heads = head_count // spread
    local_kv = max(1, kv_heads // spread)
    group_size = local_heads // local_kv
    everyone = lax.all_gather(tokens, "dp", axis=0, tiled=True)
    seq_count = everyone.shape[0]
    flat_rows = everyone.reshape(seq_count * tok_count, everyone.shape[2])
    query_cols = (
        jnp.dot(flat_rows, q_weight, preferred_element_type=jnp.float32)
        .astype(jnp.bfloat16)
        .reshape(seq_count, tok_count, -1)
    )
    key_cols = (
        jnp.dot(flat_rows, k_weight, preferred_element_type=jnp.float32)
        .astype(jnp.bfloat16)
        .reshape(seq_count, tok_count, -1)
    )
    value_cols = (
        jnp.dot(flat_rows, v_weight, preferred_element_type=jnp.float32)
        .astype(jnp.bfloat16)
        .reshape(seq_count, tok_count, -1)
    )
    query_mine, key_mine, value_mine = (
        lax.all_to_all(query_cols, "dp", split_axis=0, concat_axis=2, tiled=True),
        lax.all_to_all(key_cols, "dp", split_axis=0, concat_axis=2, tiled=True),
        lax.all_to_all(value_cols, "dp", split_axis=0, concat_axis=2, tiled=True),
    )
    queries = query_mine[0]
    keys_proj = key_mine[0]
    values_proj = value_mine[0]
    forget_input = (
        jnp.dot(own_rows, forget_weight, preferred_element_type=jnp.float32)
        + forget_offset[0][:, None]
    ).astype(jnp.bfloat16)
    query_send = queries.reshape(tok_count, spread, local_heads, head_dim)
    forget_send = forget_input.reshape(tok_count, spread, local_heads)
    if kv_heads >= spread:
        key_send = keys_proj.reshape(tok_count, spread, local_kv, head_dim)
        value_send = values_proj.reshape(tok_count, spread, local_kv, head_dim)
    else:
        copies = spread // kv_heads
        key_send = jnp.broadcast_to(
            keys_proj.reshape(tok_count, kv_heads, 1, head_dim),
            (tok_count, kv_heads, copies, head_dim),
        ).reshape(tok_count, spread, 1, head_dim)
        value_send = jnp.broadcast_to(
            values_proj.reshape(tok_count, kv_heads, 1, head_dim),
            (tok_count, kv_heads, copies, head_dim),
        ).reshape(tok_count, spread, 1, head_dim)
    query_head, forget_head, key_head, value_head = (
        lax.all_to_all(query_send, "sp", split_axis=1, concat_axis=0, tiled=True),
        lax.all_to_all(forget_send, "sp", split_axis=1, concat_axis=0, tiled=True),
        lax.all_to_all(key_send, "sp", split_axis=1, concat_axis=0, tiled=True),
        lax.all_to_all(value_send, "sp", split_axis=1, concat_axis=0, tiled=True),
    )
    length = query_head.shape[0]
    first_head = lax.axis_index("sp") * local_heads
    bias_local = lax.dynamic_slice_in_dim(forget_bias, first_head, local_heads, 0)
    gain_local = lax.dynamic_slice_in_dim(score_gain, first_head, local_heads, 0)
    norm_local = lax.dynamic_slice_in_dim(
        out_gain, first_head * head_dim, local_heads * head_dim, 0
    )
    log_gate = jax.nn.log_sigmoid(
        forget_head.reshape(length, local_heads).astype(jnp.float32) + bias_local[None, :]
    )
    cumulative = jnp.cumsum(log_gate, axis=0).reshape(length, local_kv, group_size)
    query_unit = head_norm(query_head.astype(jnp.float32), QK_FLOOR).astype(jnp.bfloat16)
    key_unit = head_norm(
        key_head.reshape(length, local_kv, head_dim).astype(jnp.float32), QK_FLOOR
    ).astype(jnp.bfloat16)
    value_heads = value_head.reshape(length, local_kv, head_dim)
    factor = (gain_local * head_dim ** (-0.5)).reshape(local_kv, group_size)
    out_gains = norm_local.reshape(local_kv, group_size, head_dim)
    key_totals = jnp.transpose(cumulative, (1, 2, 0))
    span_rows = 512
    positions = jnp.arange(length, dtype=jnp.int32)

    def attend_block(block_index):
        first = block_index * span_rows
        query_block = lax.dynamic_slice_in_dim(query_unit, first, span_rows, 0)
        query_totals = lax.dynamic_slice_in_dim(cumulative, first, span_rows, 0)
        scores = jnp.einsum(
            "qkgd,skd->kgqs", query_block, key_unit, preferred_element_type=jnp.float32
        )
        scores = (
            scores * factor[:, :, None, None]
            + jnp.transpose(query_totals, (1, 2, 0))[..., None]
            - key_totals[:, :, None, :]
        )
        allowed = positions[None, :] <= (first + jnp.arange(span_rows, dtype=jnp.int32))[:, None]
        scores = jnp.where(allowed[None, None], scores, NEG)
        row_peak = jnp.max(scores, axis=-1, keepdims=True)
        exponent = jnp.exp(scores - row_peak)
        weights = (exponent / jnp.sum(exponent, axis=-1, keepdims=True)).astype(jnp.bfloat16)
        mixed = jnp.einsum(
            "kgqs,skd->qkgd", weights, value_heads, preferred_element_type=jnp.float32
        )
        return (head_norm(mixed, OUT_FLOOR) * out_gains).astype(jnp.bfloat16)

    outputs = lax.map(attend_block, jnp.arange(length // span_rows, dtype=jnp.int32))
    outputs = outputs.reshape(length, local_heads, head_dim)
    back_rows = lax.all_to_all(outputs, "sp", split_axis=0, concat_axis=1, tiled=True)
    return back_rows.reshape(1, tok_count, head_count * head_dim)


def heads_on_dp(
    tokens,
    forget_offset,
    q_weight,
    k_weight,
    v_weight,
    forget_weight,
    forget_bias,
    score_gain,
    out_gain,
):
    tok_count = tokens.shape[1]
    head_count = forget_bias.shape[0]
    head_dim = out_gain.shape[0] // head_count
    seq_count = lax.axis_size("dp")
    kv = k_weight.shape[1] // head_dim
    heads = q_weight.shape[1] // head_dim
    group = heads // kv
    everyone = lax.all_gather(tokens, "dp", axis=0, tiled=True)
    offsets = lax.all_gather(forget_offset, "dp", axis=0, tiled=True)
    flat = everyone.reshape(seq_count * tok_count, -1)
    first = lax.axis_index("dp") * heads

    def mine(array):
        return lax.dynamic_slice_in_dim(array, first, heads, array.ndim - 1)

    def project(weight):
        return jnp.dot(flat, weight, preferred_element_type=jnp.float32).astype(jnp.bfloat16)

    key_unit = head_norm(
        project(k_weight).astype(jnp.float32).reshape(seq_count, tok_count, kv, head_dim), QK_FLOOR
    ).astype(jnp.bfloat16)
    values = project(v_weight).reshape(seq_count, tok_count, kv, head_dim)
    pair = lax.all_gather(jnp.stack([key_unit, values]), "sp", axis=2, tiled=True)
    forget_input = (
        jnp.dot(flat, mine(forget_weight), preferred_element_type=jnp.float32)
        + offsets.reshape(-1)[:, None]
    ).astype(jnp.bfloat16)
    log_gate = jax.nn.log_sigmoid(forget_input.astype(jnp.float32) + mine(forget_bias)[None, :])
    gates = lax.all_gather(
        log_gate.reshape(seq_count, tok_count, heads), "sp", axis=1, tiled=True
    )
    cumulative = jnp.cumsum(gates, axis=1)
    length = gates.shape[1]
    start = lax.axis_index("sp") * tok_count
    own = lax.dynamic_slice_in_dim(cumulative, start, tok_count, 1)
    query_unit = head_norm(
        project(q_weight).astype(jnp.float32).reshape(seq_count, tok_count, kv, group, head_dim),
        QK_FLOOR,
    ).astype(jnp.bfloat16)
    factor = (mine(score_gain) * head_dim ** (-0.5)).reshape(kv, group)
    scores = jnp.einsum(
        "bqkgd,bskd->bkgqs", query_unit, pair[0], preferred_element_type=jnp.float32
    )
    by_head = jnp.transpose(own.reshape(seq_count, tok_count, kv, group), (0, 2, 3, 1))
    by_key = jnp.transpose(cumulative.reshape(seq_count, length, kv, group), (0, 2, 3, 1))
    scores = (
        scores * factor[None, :, :, None, None] + by_head[..., None] - by_key[..., None, :]
    )
    allowed = jnp.arange(length)[None, :] <= (start + jnp.arange(tok_count))[:, None]
    scores = jnp.where(allowed, scores, NEG)
    exponent = jnp.exp(scores - jnp.max(scores, axis=-1, keepdims=True))
    weights = (exponent / jnp.sum(exponent, axis=-1, keepdims=True)).astype(jnp.bfloat16)
    mixed = jnp.einsum(
        "bkgqs,bskd->bqkgd", weights, pair[1], preferred_element_type=jnp.float32
    )
    gains = lax.dynamic_slice_in_dim(out_gain, first * head_dim, heads * head_dim, 0)
    outputs = (head_norm(mixed, OUT_FLOOR) * gains.reshape(kv, group, head_dim)).astype(
        jnp.bfloat16
    )
    outputs = outputs.reshape(seq_count, tok_count, heads * head_dim)
    return lax.all_to_all(outputs, "dp", split_axis=0, concat_axis=2, tiled=True)


LOG2E = 1.4426950408889634


def fused_kernel(
    tok_in,
    off_in,
    qw_in,
    kw_in,
    vw_in,
    fw_in,
    bias_in,
    gain_in,
    norm_in,
    result,
    tok,
    qw,
    kvw,
    fw,
    off,
    bias_row,
    gain,
    norm,
    q_unit,
    kv,
    running_all,
    gates,
    sent,
    load_sem,
    ready,
    off_send,
    off_recv,
    beside_send,
    beside_recv,
    over_send,
    over_recv,
    onward_send,
    onward_recv,
    gate_send,
    gate_recv,
    kv_send,
    kv_recv,
    back_send,
    out_send,
    out_recv,
):
    d = lax.axis_index("dp")
    s = lax.axis_index("sp")
    spread = lax.axis_size("sp")
    rows, width = tok_in.shape
    half, quarter = rows // 2, rows // 4
    cols = qw_in.shape[1]
    head_dim = kw_in.shape[1]
    heads = cols // head_dim
    seqs = tok.shape[0]
    chip, core = d // 2, d % 2
    last = spread - 1
    scope = jax.named_scope

    def peer(step):
        across = step // 2
        own_chip = (1 - across) * ((core + step % 2) % 2)
        return ((chip + across) % 2) * 2 + across * (step % 2) + own_chip

    def seen_as(step):
        return (step // 2) * (2 + core) + (1 - step // 2) * step

    def remote(src, dst, send, recv, **target):
        return pltpu.make_async_remote_copy(
            src_ref=src,
            dst_ref=dst,
            send_sem=send,
            recv_sem=recv,
            device_id=target,
            device_id_type=pl.DeviceIdType.MESH,
        )

    barrier = pltpu.get_barrier_semaphore()
    for step in range(1, seqs):
        pl.semaphore_signal(
            barrier, inc=1, device_id={"dp": peer(step)}, device_id_type=pl.DeviceIdType.MESH
        )

    @pl.when(s > 0)
    def _():
        pl.semaphore_signal(
            barrier, inc=1, device_id={"sp": s - 1}, device_id_type=pl.DeviceIdType.MESH
        )

    @pl.when(s < last)
    def _():
        pl.semaphore_signal(
            barrier, inc=1, device_id={"sp": s + 1}, device_id_type=pl.DeviceIdType.MESH
        )

    def load(src, dst, index):
        copy = pltpu.make_async_copy(src, dst, load_sem.at[index])
        copy.start()
        return copy

    load_tok = load(tok_in, tok.at[0], 0)
    load_off = load(off_in, off.at[0], 1)
    load_k = load(kw_in, kvw.at[:, pl.ds(0, head_dim)], 2)
    load_v = load(vw_in, kvw.at[:, pl.ds(head_dim, head_dim)], 3)
    load_f = load(fw_in, fw, 4)
    load_b = load(bias_in, bias_row, 5)
    load_g = load(gain_in, gain, 6)
    load_n = load(norm_in, norm, 7)
    load_q = load(qw_in, qw, 8)

    load_tok.wait()
    load_off.wait()
    with scope("bar"):
        pl.semaphore_wait(barrier, seqs - 1 + (s + last) // spread + 1 - (s + 1) // spread)

    def tell_back(target):
        pl.semaphore_signal(
            ready.at[target], inc=1, device_id={"sp": s - 1}, device_id_type=pl.DeviceIdType.MESH
        )

    @pl.when(jnp.logical_and(s > 0, s < last))
    def _():
        tell_back(s + 1)

    def await_ready(source):
        for target in range(source + 2, spread):
            pl.semaphore_wait(ready.at[target], 1)
            if source > 0:
                tell_back(target)

    offs = [
        remote(off.at[0], off.at[seen_as(step)], off_send.at[0], off_recv.at[0], dp=peer(step))
        for step in range(1, seqs)
    ]
    for copy in offs:
        copy.start()

    def half_of(index):
        return pl.ds(pl.multiple_of(index * half, half), half)

    beside = [
        remote(
            tok.at[0, half_of(part)], tok.at[1, half_of(part)], beside_send.at[0],
            beside_recv.at[i], dp=peer(1),
        )
        for i, part in enumerate((1 - core, core))
    ]
    crossings = [
        (1, 3, 0, quarter),
        (0, 2, 0, half),
        (1, 2, half, half),
        (0, 3, quarter, quarter),
        (1, 3, half, quarter),
        (1, 3, half + quarter, quarter),
    ]
    over, onward = [], []
    for j, (sender, slot, first, count) in enumerate(crossings):
        part = pl.ds(first, count)
        held = 0 if sender == slot - 2 else 1
        over.append(
            remote(
                tok.at[held, part], tok.at[slot, part], over_send.at[0], over_recv.at[j],
                dp=(1 - chip) * 2 + core,
            )
        )
        onward.append(
            remote(
                tok.at[slot, part], tok.at[slot, part], onward_send.at[0], onward_recv.at[j],
                dp=peer(1),
            )
        )

    @pl.when(core == 0)
    def _():
        over[1].start()

    @pl.when(core == 1)
    def _():
        over[0].start()

    for copy in beside:
        copy.start()

    def unit(vectors):
        vectors = vectors.astype(jnp.bfloat16).astype(jnp.float32)
        return head_norm(vectors, QK_FLOOR).astype(jnp.bfloat16)

    def returned(slot):
        return (last - 1, last - 1, 1, 0)[slot]

    def delayed(slot):
        return slot == 1

    def to_each(act):
        for target in range(last, 0, -1):

            @pl.when(s < target)
            def _():
                act(target)

    def kv_copy(slot, first, count, target):
        piece = kv.at[slot, :, pl.ds(pl.multiple_of(s * rows + first, quarter), count)]
        return remote(piece, piece, kv_send.at[target], kv_recv.at[slot, s], sp=target)

    def gate_copy(slot, target):
        piece = gates.at[slot, s]
        return remote(piece, piece, gate_send.at[target], gate_recv.at[slot], sp=target)

    def back_copy(slot, block):
        piece = kv.at[slot, :, pl.ds(block * rows, rows)]
        return remote(piece, piece, back_send.at[slot], kv_recv.at[slot, block], sp=last - 1)

    def send_kv(slot, *parts):
        def act(target):
            skip_from = last - 1 if target == last and delayed(slot) else last
            skip_below = returned(slot) if target == last - 1 else 0
            for first, count in parts:

                @pl.when(jnp.logical_and(s >= skip_below, s < skip_from))
                def _():
                    kv_copy(slot, first, count, target).start()

        to_each(act)

    def send_gate(slot):
        to_each(lambda target: gate_copy(slot, target).start())

    def project_kv(slot, *parts):
        pair = jnp.dot(
            jnp.concatenate([tok[slot, first : first + count] for first, count in parts], axis=0),
            kvw[...],
            preferred_element_type=jnp.float32,
        )
        done = 0
        for first, count in parts:
            here = pl.ds(pl.multiple_of(s * rows + first, quarter), count)
            piece = pair[done : done + count]
            kv[slot, 0, here] = unit(piece[:, :head_dim])
            kv[slot, 1, here] = piece[:, head_dim:].astype(jnp.bfloat16)
            done += count

    def project_q(slot):
        queries = jnp.dot(tok[slot], qw[...], preferred_element_type=jnp.float32)
        for h in range(heads):
            q_unit[slot, pl.ds(h * rows, rows)] = unit(
                queries[:, h * head_dim : (h + 1) * head_dim]
            )

    count = bias_in.shape[1]

    def gate(slot):
        forget_input = (
            lax.dot_general(
                fw[...], tok[slot], (((1,), (1,)), ((), ())), preferred_element_type=jnp.float32
            )
            + off[slot]
        ).astype(jnp.bfloat16)
        square = (count, count)
        diagonal = lax.broadcasted_iota(jnp.int32, square, 0) == lax.broadcasted_iota(
            jnp.int32, square, 1
        )
        bias = jnp.sum(
            jnp.where(diagonal, jnp.broadcast_to(bias_row[...], square), 0.0),
            axis=1,
            keepdims=True,
        )
        gate_arg = forget_input.astype(jnp.float32) + bias
        log_gate = jnp.minimum(gate_arg, 0.0) - jnp.log1p(jnp.exp(-jnp.abs(gate_arg)))
        before = lax.broadcasted_iota(jnp.int32, (rows, rows), 0)
        after = lax.broadcasted_iota(jnp.int32, (rows, rows), 1)
        upto = (before <= after).astype(jnp.bfloat16)
        high = log_gate.astype(jnp.bfloat16)
        rest = log_gate - high.astype(jnp.float32)
        middle = rest.astype(jnp.bfloat16)
        low = (rest - middle.astype(jnp.float32)).astype(jnp.bfloat16)
        running = (
            jnp.dot(low, upto, preferred_element_type=jnp.float32)
            + jnp.dot(middle, upto, preferred_element_type=jnp.float32)
            + jnp.dot(high, upto, preferred_element_type=jnp.float32)
        )
        running_all[...] = running * LOG2E
        own = running_all[pl.ds(d * heads, heads)]
        spare = gates.shape[2] - heads
        if spare:
            own = jnp.concatenate([own, jnp.zeros((spare, rows), jnp.float32)], axis=0)
        gates[slot, s] = own

    def out_copy(slot, start, group):
        place = pl.ds(
            pl.multiple_of(d * cols + start * head_dim, head_dim), group * head_dim
        )
        return remote(
            sent.at[slot, :, pl.ds(start * head_dim, group * head_dim)], result.at[:, place],
            out_send.at[0], out_recv.at[0], dp=peer(slot),
        )

    def attend(slot, blocks, group):
        span = blocks * rows
        later = jnp.zeros((gates.shape[2], 1), jnp.float32)
        totals = [gates[slot, blocks - 1]]
        for b in range(blocks - 2, -1, -1):
            local_sum = gates[slot, b]
            later = later + local_sum[:, rows - 1 :]
            totals.insert(0, local_sum - later)
        allowed = lax.broadcasted_iota(jnp.int32, (rows, rows), 1) <= lax.broadcasted_iota(
            jnp.int32, (rows, rows), 0
        )
        keys = kv[slot, 0, :span]
        values = kv[slot, 1, :span]
        for start in range(0, heads, group):
            each = range(start, start + group)
            raw = [
                lax.dot_general(
                    q_unit[slot, pl.ds(h * rows, rows)],
                    keys,
                    (((1,), (1,)), ((), ())),
                    preferred_element_type=jnp.float32,
                )
                for h in each
            ]
            scores = []
            for h, product in zip(each, raw):
                factor = gain[0, d * heads + h] * (head_dim ** (-0.5) * LOG2E)
                parts = [
                    product[:, b * rows : (b + 1) * rows] * factor - totals[b][h : h + 1, :]
                    for b in range(blocks)
                ]
                parts[-1] = jnp.where(allowed, parts[-1], NEG)
                scores.append(parts)
            peaks = [
                jnp.max(functools.reduce(jnp.maximum, parts), axis=-1, keepdims=True)
                for parts in scores
            ]
            exponents = [
                [jnp.exp2(part - peak) for part in parts] for parts, peak in zip(scores, peaks)
            ]
            scales = [
                1.0 / jnp.sum(functools.reduce(jnp.add, parts), axis=-1, keepdims=True)
                for parts in exponents
            ]
            weights = [
                jnp.concatenate([(part * scale).astype(jnp.bfloat16) for part in parts], axis=1)
                for parts, scale in zip(exponents, scales)
            ]
            mixed = [jnp.dot(w, values, preferred_element_type=jnp.float32) for w in weights]
            for h, rough in zip(each, mixed):
                place = pl.ds(pl.multiple_of(d * cols + h * head_dim, head_dim), head_dim)
                outcome = (head_norm(rough, OUT_FLOOR) * norm[:, place]).astype(jnp.bfloat16)
                if slot == 0:
                    result[:, place] = outcome
                else:
                    sent[slot, :, h * head_dim : (h + 1) * head_dim] = outcome
            if slot > 0:
                out_copy(slot, start, group).start()

    def arrived(ref, semaphore):
        pltpu.make_async_copy(ref, ref, semaphore).wait()

    def await_kv(slot, blocks):
        for b in blocks:
            arrived(kv.at[slot, :, pl.ds(b * rows, rows)], kv_recv.at[slot, b])

    def send_back(slot):
        @pl.when(s == last)
        def _():
            with scope(f"bk{slot}"):
                await_kv(slot, range(returned(slot)))
            for b in range(returned(slot)):
                back_copy(slot, b).start()

    def attend_at(slot, places):
        for k in places:

            @pl.when(s == k)
            def _():
                if k > 0:
                    with scope(f"wkv{slot}"):
                        arrived(gates.at[slot, pl.ds(0, k)], gate_recv.at[slot])
                        await_kv(slot, range(returned(slot) if k == last else 0, k))
                with scope(f"att{slot}"):
                    attend(slot, k + 1, heads // 2 if slot == seqs - 1 and heads % 2 == 0 else heads)

    def direct(j):
        with scope(f"wx{j}"):
            over[j].wait_recv()
        onward[j].start()

    def passed(j):
        with scope(f"wo{j}"):
            onward[j].wait_recv()

    def whole(j):
        return crossings[j][2:]

    def treat(slot, *js, ends=False):
        parts = [whole(j) for j in js]
        with scope(f"p{slot}" + "".join(map(str, js))):
            project_kv(slot, *parts)
            if ends:
                gate(slot)
        if ends:
            send_gate(slot)
        send_kv(slot, *parts)

    load_k.wait()
    load_v.wait()
    with scope("pkv0"):
        project_kv(0, (0, rows))
    for source in range(1, spread - 1):

        @pl.when(s == source)
        def _():
            await_ready(source)

    @pl.when(s > 0)
    def _():
        send_kv(0, (0, rows))

    with scope("wb0"):
        beside[0].wait_recv()

    @pl.when(core == 0)
    def _():
        over[3].start()

    @pl.when(core == 1)
    def _():
        over[2].start()
        over[4].start()
        over[5].start()

    load_f.wait()
    load_b.wait()
    with scope("wb1"):
        beside[1].wait_recv()
    with scope("pkv1g0"):
        gate(0)
        project_kv(1, (0, rows))

    @pl.when(s == 0)
    def _():
        with scope("rdy"):
            await_ready(0)
        send_kv(0, (0, rows))

    send_gate(0)
    send_kv(1, (0, rows))
    load_q.wait()
    load_g.wait()
    load_n.wait()
    with scope("woff"):
        arrived(off.at[pl.ds(1, seqs - 1)], off_recv.at[0])
    with scope("pq01g1"):
        gate(1)
        project_q(0)
        project_q(1)
    send_gate(1)

    @pl.when(core == 0)
    def _():
        passed(0)
        treat(3, 0)
        send_back(0)
        direct(1)
        treat(2, 1)
        send_back(1)
        passed(2)
        treat(2, 2, ends=True)

    @pl.when(core == 1)
    def _():
        direct(0)
        treat(3, 0)
        send_back(0)
        direct(2)
        treat(2, 2)
        send_back(1)
        passed(1)
        treat(2, 1, ends=True)

    with scope("pq2"):
        project_q(2)
    attend_at(2, [0])
    attend_at(0, [last])

    @pl.when(core == 0)
    def _():
        direct(3)
        treat(3, 3)
        passed(4)
        treat(3, 4)
        passed(5)
        treat(3, 5, ends=True)

    @pl.when(core == 1)
    def _():
        direct(4)
        treat(3, 4)
        direct(5)
        passed(3)
        treat(3, 3, 5, ends=True)

    for slot in range(seqs):
        if delayed(slot):

            @pl.when(s == last - 1)
            def _():
                kv_copy(slot, 0, rows, last).start()

    send_back(2)
    with scope("pq3"):
        project_q(3)
    attend_at(3, [0])
    attend_at(0, [last - 1])
    attend_at(1, [last - 1])
    attend_at(2, range(1, spread))
    attend_at(0, range(last - 1))
    attend_at(1, range(last - 1))
    attend_at(3, range(1, spread))
    attend_at(1, [last])

    with scope("flush"):
        arrived(sent.at[pl.ds(1, seqs - 1)], out_recv.at[0])
    with scope("drain"):
        arrived(sent.at[pl.ds(1, seqs - 1)], out_send.at[0])
        arrived(off.at[pl.ds(1, seqs - 1)], off_send.at[0])
        arrived(tok.at[0], beside_send.at[0])
        for sender in range(2):
            many = sum(item[3] for item in crossings if item[0] == sender)

            @pl.when(core == sender)
            def _():
                for semaphore in (over_send, onward_send):
                    arrived(tok.at[pl.ds(0, 2), pl.ds(0, many // 2)], semaphore.at[0])

        def sent_to(target):
            arrived(gates.at[pl.ds(0, seqs), 0], gate_send.at[target])
            for source in range(target):
                skipped = sum(
                    target == last - 1 and source < returned(slot) for slot in range(seqs)
                )

                @pl.when(s == source)
                def _():
                    arrived(
                        kv.at[pl.ds(skipped, seqs - skipped), :, pl.ds(0, rows)],
                        kv_send.at[target],
                    )

        to_each(sent_to)

        @pl.when(s == last)
        def _():
            for slot in range(seqs):
                if returned(slot):
                    arrived(kv.at[slot, :, pl.ds(0, returned(slot) * rows)], back_send.at[slot])


def fused(
    tokens,
    forget_offset,
    q_weight,
    k_weight,
    v_weight,
    forget_weight,
    forget_bias,
    score_gain,
    out_gain,
):
    rows, width = tokens.shape[1:]
    head_count = forget_bias.shape[0]
    head_dim = out_gain.shape[0] // head_count
    seqs = lax.axis_size("dp")
    spread = lax.axis_size("sp")
    cols = q_weight.shape[1]
    heads = cols // head_dim
    padded = -(-heads // 8) * 8
    outside = pl.BlockSpec(memory_space=pltpu.HBM)
    dma = pltpu.SemaphoreType.DMA
    out = pl.pallas_call(
        fused_kernel,
        out_shape=pltpu.VMEM((rows, seqs * cols), jnp.bfloat16),
        in_specs=[outside] * 9,
        out_specs=pl.BlockSpec(memory_space=pltpu.VMEM),
        scratch_shapes=[
            pltpu.VMEM((seqs, rows, width), jnp.bfloat16),
            pltpu.VMEM((width, cols), jnp.bfloat16),
            pltpu.VMEM((width, 2 * head_dim), jnp.bfloat16),
            pltpu.VMEM((head_count, width), jnp.bfloat16),
            pltpu.VMEM((seqs, 1, rows), jnp.float32),
            pltpu.VMEM((1, head_count), jnp.float32),
            pltpu.SMEM((1, head_count), jnp.float32),
            pltpu.VMEM((1, head_count * head_dim), jnp.float32),
            pltpu.VMEM((seqs, heads * rows, head_dim), jnp.bfloat16),
            pltpu.VMEM((seqs, 2, spread * rows, head_dim), jnp.bfloat16),
            pltpu.VMEM((head_count, rows), jnp.float32),
            pltpu.VMEM((seqs, spread, padded, rows), jnp.float32),
            pltpu.VMEM((seqs, rows, cols), jnp.bfloat16),
            dma((9,)),
            pltpu.SemaphoreType.REGULAR((spread,)),
            dma((1,)),
            dma((1,)),
            dma((1,)),
            dma((2,)),
            dma((1,)),
            dma((6,)),
            dma((1,)),
            dma((6,)),
            dma((spread,)),
            dma((seqs,)),
            dma((spread,)),
            dma((seqs, spread)),
            dma((seqs,)),
            dma((1,)),
            dma((1,)),
        ],
        compiler_params=pltpu.CompilerParams(
            collective_id=0, has_side_effects=True
        ),
    )(
        tokens[0],
        forget_offset,
        q_weight,
        k_weight,
        v_weight,
        forget_weight.T,
        forget_bias[None, :],
        score_gain[None, :],
        out_gain[None, :],
    )
    return out[None]


def local(*args):
    tokens, k_weight, forget_bias, out_gain = args[0], args[3], args[6], args[8]
    head_dim = out_gain.shape[0] // forget_bias.shape[0]
    fits = tokens.shape[0] == 1 and tokens.shape[1] % 128 == 0 and head_dim % 128 == 0
    if (
        lax.axis_size("dp") == 4
        and 2 < lax.axis_size("sp") <= 4
        and k_weight.shape[1] == head_dim
        and fits
    ):
        return fused(*args)
    if k_weight.shape[1] % head_dim == 0 and tokens.shape[0] == 1:
        return heads_on_dp(*args)
    return heads_on_sp(*args)


def solution(mesh):
    in_specs = (
        P(("grp", "dp"), "sp", None),
        P(("grp", "dp"), "sp"),
        P(None, "dp"),
        P(None, "dp"),
        P(None, "dp"),
        P(),
        P(),
        P(),
        P(),
    )
    out_specs = P(("grp", "dp"), "sp", None)
    return jax.shard_map(local, mesh=mesh, in_specs=in_specs, out_specs=out_specs, check_vma=False)
```

```python
import functools

import jax
import jax.numpy as jnp
from jax import lax
from jax.experimental import pallas as pl
from jax.experimental.pallas import tpu as pltpu
from jax.sharding import PartitionSpec as P

NEG = -1e30
QK_FLOOR = 0.1
OUT_FLOOR = 0.001


def head_norm(vectors, floor):
    return vectors * lax.rsqrt(jnp.mean(vectors * vectors, axis=-1, keepdims=True) + floor)


def heads_on_sp(
    tokens,
    forget_offset,
    q_weight,
    k_weight,
    v_weight,
    forget_weight,
    forget_bias,
    score_gain,
    out_gain,
):
    own_rows = tokens[0]
    tok_count = own_rows.shape[0]
    head_count = forget_bias.shape[0]
    head_dim = out_gain.shape[0] // head_count
    kv_heads = k_weight.shape[1] * lax.axis_size("dp") // head_dim
    spread = lax.axis_size("sp")
    local_heads = head_count // spread
    local_kv = max(1, kv_heads // spread)
    group_size = local_heads // local_kv
    everyone = lax.all_gather(tokens, "dp", axis=0, tiled=True)
    seq_count = everyone.shape[0]
    flat_rows = everyone.reshape(seq_count * tok_count, everyone.shape[2])
    query_cols = (
        jnp.dot(flat_rows, q_weight, preferred_element_type=jnp.float32)
        .astype(jnp.bfloat16)
        .reshape(seq_count, tok_count, -1)
    )
    key_cols = (
        jnp.dot(flat_rows, k_weight, preferred_element_type=jnp.float32)
        .astype(jnp.bfloat16)
        .reshape(seq_count, tok_count, -1)
    )
    value_cols = (
        jnp.dot(flat_rows, v_weight, preferred_element_type=jnp.float32)
        .astype(jnp.bfloat16)
        .reshape(seq_count, tok_count, -1)
    )
    query_mine, key_mine, value_mine = (
        lax.all_to_all(query_cols, "dp", split_axis=0, concat_axis=2, tiled=True),
        lax.all_to_all(key_cols, "dp", split_axis=0, concat_axis=2, tiled=True),
        lax.all_to_all(value_cols, "dp", split_axis=0, concat_axis=2, tiled=True),
    )
    queries = query_mine[0]
    keys_proj = key_mine[0]
    values_proj = value_mine[0]
    forget_input = (
        jnp.dot(own_rows, forget_weight, preferred_element_type=jnp.float32)
        + forget_offset[0][:, None]
    ).astype(jnp.bfloat16)
    query_send = queries.reshape(tok_count, spread, local_heads, head_dim)
    forget_send = forget_input.reshape(tok_count, spread, local_heads)
    if kv_heads >= spread:
        key_send = keys_proj.reshape(tok_count, spread, local_kv, head_dim)
        value_send = values_proj.reshape(tok_count, spread, local_kv, head_dim)
    else:
        copies = spread // kv_heads
        key_send = jnp.broadcast_to(
            keys_proj.reshape(tok_count, kv_heads, 1, head_dim),
            (tok_count, kv_heads, copies, head_dim),
        ).reshape(tok_count, spread, 1, head_dim)
        value_send = jnp.broadcast_to(
            values_proj.reshape(tok_count, kv_heads, 1, head_dim),
            (tok_count, kv_heads, copies, head_dim),
        ).reshape(tok_count, spread, 1, head_dim)
    query_head, forget_head, key_head, value_head = (
        lax.all_to_all(query_send, "sp", split_axis=1, concat_axis=0, tiled=True),
        lax.all_to_all(forget_send, "sp", split_axis=1, concat_axis=0, tiled=True),
        lax.all_to_all(key_send, "sp", split_axis=1, concat_axis=0, tiled=True),
        lax.all_to_all(value_send, "sp", split_axis=1, concat_axis=0, tiled=True),
    )
    length = query_head.shape[0]
    first_head = lax.axis_index("sp") * local_heads
    bias_local = lax.dynamic_slice_in_dim(forget_bias, first_head, local_heads, 0)
    gain_local = lax.dynamic_slice_in_dim(score_gain, first_head, local_heads, 0)
    norm_local = lax.dynamic_slice_in_dim(
        out_gain, first_head * head_dim, local_heads * head_dim, 0
    )
    log_gate = jax.nn.log_sigmoid(
        forget_head.reshape(length, local_heads).astype(jnp.float32) + bias_local[None, :]
    )
    cumulative = jnp.cumsum(log_gate, axis=0).reshape(length, local_kv, group_size)
    query_unit = head_norm(query_head.astype(jnp.float32), QK_FLOOR).astype(jnp.bfloat16)
    key_unit = head_norm(
        key_head.reshape(length, local_kv, head_dim).astype(jnp.float32), QK_FLOOR
    ).astype(jnp.bfloat16)
    value_heads = value_head.reshape(length, local_kv, head_dim)
    factor = (gain_local * head_dim ** (-0.5)).reshape(local_kv, group_size)
    out_gains = norm_local.reshape(local_kv, group_size, head_dim)
    key_totals = jnp.transpose(cumulative, (1, 2, 0))
    span_rows = 512
    positions = jnp.arange(length, dtype=jnp.int32)

    def attend_block(block_index):
        first = block_index * span_rows
        query_block = lax.dynamic_slice_in_dim(query_unit, first, span_rows, 0)
        query_totals = lax.dynamic_slice_in_dim(cumulative, first, span_rows, 0)
        scores = jnp.einsum(
            "qkgd,skd->kgqs", query_block, key_unit, preferred_element_type=jnp.float32
        )
        scores = (
            scores * factor[:, :, None, None]
            + jnp.transpose(query_totals, (1, 2, 0))[..., None]
            - key_totals[:, :, None, :]
        )
        allowed = positions[None, :] <= (first + jnp.arange(span_rows, dtype=jnp.int32))[:, None]
        scores = jnp.where(allowed[None, None], scores, NEG)
        row_peak = jnp.max(scores, axis=-1, keepdims=True)
        exponent = jnp.exp(scores - row_peak)
        weights = (exponent / jnp.sum(exponent, axis=-1, keepdims=True)).astype(jnp.bfloat16)
        mixed = jnp.einsum(
            "kgqs,skd->qkgd", weights, value_heads, preferred_element_type=jnp.float32
        )
        return (head_norm(mixed, OUT_FLOOR) * out_gains).astype(jnp.bfloat16)

    outputs = lax.map(attend_block, jnp.arange(length // span_rows, dtype=jnp.int32))
    outputs = outputs.reshape(length, local_heads, head_dim)
    back_rows = lax.all_to_all(outputs, "sp", split_axis=0, concat_axis=1, tiled=True)
    return back_rows.reshape(1, tok_count, head_count * head_dim)


def heads_on_dp(
    tokens,
    forget_offset,
    q_weight,
    k_weight,
    v_weight,
    forget_weight,
    forget_bias,
    score_gain,
    out_gain,
):
    tok_count = tokens.shape[1]
    head_count = forget_bias.shape[0]
    head_dim = out_gain.shape[0] // head_count
    seq_count = lax.axis_size("dp")
    kv = k_weight.shape[1] // head_dim
    heads = q_weight.shape[1] // head_dim
    group = heads // kv
    everyone = lax.all_gather(tokens, "dp", axis=0, tiled=True)
    offsets = lax.all_gather(forget_offset, "dp", axis=0, tiled=True)
    flat = everyone.reshape(seq_count * tok_count, -1)
    first = lax.axis_index("dp") * heads

    def mine(array):
        return lax.dynamic_slice_in_dim(array, first, heads, array.ndim - 1)

    def project(weight):
        return jnp.dot(flat, weight, preferred_element_type=jnp.float32).astype(jnp.bfloat16)

    key_unit = head_norm(
        project(k_weight).astype(jnp.float32).reshape(seq_count, tok_count, kv, head_dim), QK_FLOOR
    ).astype(jnp.bfloat16)
    values = project(v_weight).reshape(seq_count, tok_count, kv, head_dim)
    pair = lax.all_gather(jnp.stack([key_unit, values]), "sp", axis=2, tiled=True)
    forget_input = (
        jnp.dot(flat, mine(forget_weight), preferred_element_type=jnp.float32)
        + offsets.reshape(-1)[:, None]
    ).astype(jnp.bfloat16)
    log_gate = jax.nn.log_sigmoid(forget_input.astype(jnp.float32) + mine(forget_bias)[None, :])
    gates = lax.all_gather(
        log_gate.reshape(seq_count, tok_count, heads), "sp", axis=1, tiled=True
    )
    cumulative = jnp.cumsum(gates, axis=1)
    length = gates.shape[1]
    start = lax.axis_index("sp") * tok_count
    own = lax.dynamic_slice_in_dim(cumulative, start, tok_count, 1)
    query_unit = head_norm(
        project(q_weight).astype(jnp.float32).reshape(seq_count, tok_count, kv, group, head_dim),
        QK_FLOOR,
    ).astype(jnp.bfloat16)
    factor = (mine(score_gain) * head_dim ** (-0.5)).reshape(kv, group)
    scores = jnp.einsum(
        "bqkgd,bskd->bkgqs", query_unit, pair[0], preferred_element_type=jnp.float32
    )
    by_head = jnp.transpose(own.reshape(seq_count, tok_count, kv, group), (0, 2, 3, 1))
    by_key = jnp.transpose(cumulative.reshape(seq_count, length, kv, group), (0, 2, 3, 1))
    scores = (
        scores * factor[None, :, :, None, None] + by_head[..., None] - by_key[..., None, :]
    )
    allowed = jnp.arange(length)[None, :] <= (start + jnp.arange(tok_count))[:, None]
    scores = jnp.where(allowed, scores, NEG)
    exponent = jnp.exp(scores - jnp.max(scores, axis=-1, keepdims=True))
    weights = (exponent / jnp.sum(exponent, axis=-1, keepdims=True)).astype(jnp.bfloat16)
    mixed = jnp.einsum(
        "bkgqs,bskd->bqkgd", weights, pair[1], preferred_element_type=jnp.float32
    )
    gains = lax.dynamic_slice_in_dim(out_gain, first * head_dim, heads * head_dim, 0)
    outputs = (head_norm(mixed, OUT_FLOOR) * gains.reshape(kv, group, head_dim)).astype(
        jnp.bfloat16
    )
    outputs = outputs.reshape(seq_count, tok_count, heads * head_dim)
    return lax.all_to_all(outputs, "dp", split_axis=0, concat_axis=2, tiled=True)


LOG2E = 1.4426950408889634


def fused_kernel(
    tok_in,
    off_in,
    qw_in,
    kw_in,
    vw_in,
    fw_in,
    bias_in,
    gain_in,
    norm_in,
    result,
    tok,
    qw,
    kvw,
    fw,
    off,
    bias_row,
    gain,
    norm,
    q_unit,
    kv,
    running_all,
    gates,
    sent,
    load_sem,
    ready,
    off_send,
    off_recv,
    beside_send,
    beside_recv,
    over_send,
    over_recv,
    onward_send,
    onward_recv,
    gate_send,
    gate_recv,
    kv_send,
    kv_recv,
    back_send,
    out_send,
    out_recv,
):
    d = lax.axis_index("dp")
    s = lax.axis_index("sp")
    spread = lax.axis_size("sp")
    rows, width = tok_in.shape
    half, quarter = rows // 2, rows // 4
    cols = qw_in.shape[1]
    head_dim = kw_in.shape[1]
    heads = cols // head_dim
    seqs = tok.shape[0]
    chip, core = d // 2, d % 2
    last = spread - 1
    scope = jax.named_scope

    def peer(step):
        across = step // 2
        own_chip = (1 - across) * ((core + step % 2) % 2)
        return ((chip + across) % 2) * 2 + across * (step % 2) + own_chip

    def seen_as(step):
        return (step // 2) * (2 + core) + (1 - step // 2) * step

    def remote(src, dst, send, recv, **target):
        return pltpu.make_async_remote_copy(
            src_ref=src,
            dst_ref=dst,
            send_sem=send,
            recv_sem=recv,
            device_id=target,
            device_id_type=pl.DeviceIdType.MESH,
        )

    barrier = pltpu.get_barrier_semaphore()
    for step in range(1, seqs):
        pl.semaphore_signal(
            barrier, inc=1, device_id={"dp": peer(step)}, device_id_type=pl.DeviceIdType.MESH
        )

    @pl.when(s > 0)
    def _():
        pl.semaphore_signal(
            barrier, inc=1, device_id={"sp": s - 1}, device_id_type=pl.DeviceIdType.MESH
        )

    @pl.when(s < last)
    def _():
        pl.semaphore_signal(
            barrier, inc=1, device_id={"sp": s + 1}, device_id_type=pl.DeviceIdType.MESH
        )

    def load(src, dst, index):
        copy = pltpu.make_async_copy(src, dst, load_sem.at[index])
        copy.start()
        return copy

    load_tok = load(tok_in, tok.at[0], 0)
    load_off = load(off_in, off.at[0], 1)
    load_k = load(kw_in, kvw.at[:, pl.ds(0, head_dim)], 2)
    load_v = load(vw_in, kvw.at[:, pl.ds(head_dim, head_dim)], 3)
    load_f = load(fw_in, fw, 4)
    load_b = load(bias_in, bias_row, 5)
    load_g = load(gain_in, gain, 6)
    load_n = load(norm_in, norm, 7)
    load_q = load(qw_in, qw, 8)

    load_tok.wait()
    load_off.wait()
    with scope("bar"):
        pl.semaphore_wait(barrier, seqs - 1 + (s + last) // spread + 1 - (s + 1) // spread)

    def tell_back(target):
        pl.semaphore_signal(
            ready.at[target], inc=1, device_id={"sp": s - 1}, device_id_type=pl.DeviceIdType.MESH
        )

    @pl.when(jnp.logical_and(s > 0, s < last))
    def _():
        tell_back(s + 1)

    def await_ready(source):
        for target in range(source + 2, spread):
            pl.semaphore_wait(ready.at[target], 1)
            if source > 0:
                tell_back(target)

    offs = [
        remote(off.at[0], off.at[seen_as(step)], off_send.at[0], off_recv.at[0], dp=peer(step))
        for step in range(1, seqs)
    ]
    for copy in offs:
        copy.start()

    def half_of(index):
        return pl.ds(pl.multiple_of(index * half, half), half)

    beside = [
        remote(
            tok.at[0, half_of(part)], tok.at[1, half_of(part)], beside_send.at[0],
            beside_recv.at[i], dp=peer(1),
        )
        for i, part in enumerate((1 - core, core))
    ]
    crossings = [
        (1, 3, 0, quarter),
        (0, 2, 0, half),
        (1, 2, half, half),
        (0, 3, quarter, quarter),
        (1, 3, half, quarter),
        (1, 3, half + quarter, quarter),
    ]
    over, onward = [], []
    for j, (sender, slot, first, count) in enumerate(crossings):
        part = pl.ds(first, count)
        held = 0 if sender == slot - 2 else 1
        over.append(
            remote(
                tok.at[held, part], tok.at[slot, part], over_send.at[0], over_recv.at[j],
                dp=(1 - chip) * 2 + core,
            )
        )
        onward.append(
            remote(
                tok.at[slot, part], tok.at[slot, part], onward_send.at[0], onward_recv.at[j],
                dp=peer(1),
            )
        )

    @pl.when(core == 0)
    def _():
        over[1].start()

    @pl.when(core == 1)
    def _():
        over[0].start()

    for copy in beside:
        copy.start()

    def unit(vectors):
        vectors = vectors.astype(jnp.bfloat16).astype(jnp.float32)
        return head_norm(vectors, QK_FLOOR).astype(jnp.bfloat16)

    def returned(slot):
        return (last - 1, last - 1, 1, 1)[slot]

    def delayed(slot):
        return slot == 1

    def to_each(act):
        for target in range(last, 0, -1):

            @pl.when(s < target)
            def _():
                act(target)

    def kv_copy(slot, first, count, target):
        piece = kv.at[slot, :, pl.ds(pl.multiple_of(s * rows + first, quarter), count)]
        return remote(piece, piece, kv_send.at[target], kv_recv.at[slot, s], sp=target)

    def gate_copy(slot, target):
        piece = gates.at[slot, s]
        return remote(piece, piece, gate_send.at[target], gate_recv.at[slot], sp=target)

    def back_copy(slot, block):
        piece = kv.at[slot, :, pl.ds(block * rows, rows)]
        return remote(piece, piece, back_send.at[slot], kv_recv.at[slot, block], sp=last - 1)

    def send_kv(slot, *parts):
        def act(target):
            skip_from = last - 1 if target == last and delayed(slot) else last
            skip_below = returned(slot) if target == last - 1 else 0
            for first, count in parts:

                @pl.when(jnp.logical_and(s >= skip_below, s < skip_from))
                def _():
                    kv_copy(slot, first, count, target).start()

        to_each(act)

    def send_gate(slot):
        to_each(lambda target: gate_copy(slot, target).start())

    def project_kv(slot, *parts):
        pair = jnp.dot(
            jnp.concatenate([tok[slot, first : first + count] for first, count in parts], axis=0),
            kvw[...],
            preferred_element_type=jnp.float32,
        )
        done = 0
        for first, count in parts:
            here = pl.ds(pl.multiple_of(s * rows + first, quarter), count)
            piece = pair[done : done + count]
            kv[slot, 0, here] = unit(piece[:, :head_dim])
            kv[slot, 1, here] = piece[:, head_dim:].astype(jnp.bfloat16)
            done += count

    def project_q(slot):
        queries = jnp.dot(tok[slot], qw[...], preferred_element_type=jnp.float32)
        for h in range(heads):
            q_unit[slot, pl.ds(h * rows, rows)] = unit(
                queries[:, h * head_dim : (h + 1) * head_dim]
            )

    count = bias_in.shape[1]

    def gate(slot):
        forget_input = (
            lax.dot_general(
                fw[...], tok[slot], (((1,), (1,)), ((), ())), preferred_element_type=jnp.float32
            )
            + off[slot]
        ).astype(jnp.bfloat16)
        square = (count, count)
        diagonal = lax.broadcasted_iota(jnp.int32, square, 0) == lax.broadcasted_iota(
            jnp.int32, square, 1
        )
        bias = jnp.sum(
            jnp.where(diagonal, jnp.broadcast_to(bias_row[...], square), 0.0),
            axis=1,
            keepdims=True,
        )
        gate_arg = forget_input.astype(jnp.float32) + bias
        log_gate = jnp.minimum(gate_arg, 0.0) - jnp.log1p(jnp.exp(-jnp.abs(gate_arg)))
        before = lax.broadcasted_iota(jnp.int32, (rows, rows), 0)
        after = lax.broadcasted_iota(jnp.int32, (rows, rows), 1)
        upto = (before <= after).astype(jnp.bfloat16)
        high = log_gate.astype(jnp.bfloat16)
        rest = log_gate - high.astype(jnp.float32)
        middle = rest.astype(jnp.bfloat16)
        low = (rest - middle.astype(jnp.float32)).astype(jnp.bfloat16)
        running = (
            jnp.dot(low, upto, preferred_element_type=jnp.float32)
            + jnp.dot(middle, upto, preferred_element_type=jnp.float32)
            + jnp.dot(high, upto, preferred_element_type=jnp.float32)
        )
        running_all[...] = running * LOG2E
        own = running_all[pl.ds(d * heads, heads)]
        spare = gates.shape[2] - heads
        if spare:
            own = jnp.concatenate([own, jnp.zeros((spare, rows), jnp.float32)], axis=0)
        gates[slot, s] = own

    def out_copy(slot, start, group):
        place = pl.ds(
            pl.multiple_of(d * cols + start * head_dim, head_dim), group * head_dim
        )
        return remote(
            sent.at[slot, :, pl.ds(start * head_dim, group * head_dim)], result.at[:, place],
            out_send.at[0], out_recv.at[0], dp=peer(slot),
        )

    def attend(slot, blocks, group):
        span = blocks * rows
        later = jnp.zeros((gates.shape[2], 1), jnp.float32)
        totals = [gates[slot, blocks - 1]]
        for b in range(blocks - 2, -1, -1):
            local_sum = gates[slot, b]
            later = later + local_sum[:, rows - 1 :]
            totals.insert(0, local_sum - later)
        allowed = lax.broadcasted_iota(jnp.int32, (rows, rows), 1) <= lax.broadcasted_iota(
            jnp.int32, (rows, rows), 0
        )
        keys = kv[slot, 0, :span]
        values = kv[slot, 1, :span]
        for start in range(0, heads, group):
            each = range(start, start + group)
            raw = [
                lax.dot_general(
                    q_unit[slot, pl.ds(h * rows, rows)],
                    keys,
                    (((1,), (1,)), ((), ())),
                    preferred_element_type=jnp.float32,
                )
                for h in each
            ]
            scores = []
            for h, product in zip(each, raw):
                factor = gain[0, d * heads + h] * (head_dim ** (-0.5) * LOG2E)
                parts = [
                    product[:, b * rows : (b + 1) * rows] * factor - totals[b][h : h + 1, :]
                    for b in range(blocks)
                ]
                parts[-1] = jnp.where(allowed, parts[-1], NEG)
                scores.append(parts)
            peaks = [
                jnp.max(functools.reduce(jnp.maximum, parts), axis=-1, keepdims=True)
                for parts in scores
            ]
            exponents = [
                [jnp.exp2(part - peak) for part in parts] for parts, peak in zip(scores, peaks)
            ]
            scales = [
                1.0 / jnp.sum(functools.reduce(jnp.add, parts), axis=-1, keepdims=True)
                for parts in exponents
            ]
            weights = [
                jnp.concatenate([(part * scale).astype(jnp.bfloat16) for part in parts], axis=1)
                for parts, scale in zip(exponents, scales)
            ]
            mixed = [jnp.dot(w, values, preferred_element_type=jnp.float32) for w in weights]
            for h, rough in zip(each, mixed):
                place = pl.ds(pl.multiple_of(d * cols + h * head_dim, head_dim), head_dim)
                outcome = (head_norm(rough, OUT_FLOOR) * norm[:, place]).astype(jnp.bfloat16)
                if slot == 0:
                    result[:, place] = outcome
                else:
                    sent[slot, :, h * head_dim : (h + 1) * head_dim] = outcome
            if slot > 0:
                out_copy(slot, start, group).start()

    def arrived(ref, semaphore):
        pltpu.make_async_copy(ref, ref, semaphore).wait()

    def await_kv(slot, blocks):
        for b in blocks:
            arrived(kv.at[slot, :, pl.ds(b * rows, rows)], kv_recv.at[slot, b])

    def send_back(slot):
        @pl.when(s == last)
        def _():
            with scope(f"bk{slot}"):
                await_kv(slot, range(returned(slot)))
            for b in range(returned(slot)):
                back_copy(slot, b).start()

    def attend_at(slot, places):
        for k in places:

            @pl.when(s == k)
            def _():
                if k > 0:
                    with scope(f"wkv{slot}"):
                        arrived(gates.at[slot, pl.ds(0, k)], gate_recv.at[slot])
                        await_kv(slot, range(returned(slot) if k == last else 0, k))
                with scope(f"att{slot}"):
                    attend(slot, k + 1, heads // 2 if slot == seqs - 1 and heads % 2 == 0 else heads)

    def direct(j):
        with scope(f"wx{j}"):
            over[j].wait_recv()
        onward[j].start()

    def passed(j):
        with scope(f"wo{j}"):
            onward[j].wait_recv()

    def whole(j):
        return crossings[j][2:]

    def treat(slot, *js, ends=False, hold=False):
        parts = [whole(j) for j in js]
        with scope(f"p{slot}" + "".join(map(str, js))):
            project_kv(slot, *parts)
            if ends:
                gate(slot)
        if ends:
            send_gate(slot)
        if not hold:
            send_kv(slot, *parts)

    load_k.wait()
    load_v.wait()
    with scope("pkv0"):
        project_kv(0, (0, rows))
    for source in range(1, spread - 1):

        @pl.when(s == source)
        def _():
            await_ready(source)

    @pl.when(s > 0)
    def _():
        send_kv(0, (0, rows))

    with scope("wb0"):
        beside[0].wait_recv()

    @pl.when(core == 0)
    def _():
        over[3].start()

    @pl.when(core == 1)
    def _():
        over[2].start()
        over[4].start()
        over[5].start()

    load_f.wait()
    load_b.wait()
    with scope("wb1"):
        beside[1].wait_recv()
    with scope("pkv1g0"):
        gate(0)
        project_kv(1, (0, rows))

    @pl.when(s == 0)
    def _():
        with scope("rdy"):
            await_ready(0)
        send_kv(0, (0, rows))

    send_gate(0)
    send_kv(1, (0, rows))
    load_q.wait()
    load_g.wait()
    load_n.wait()
    with scope("woff"):
        arrived(off.at[pl.ds(1, seqs - 1)], off_recv.at[0])
    with scope("pq01g1"):
        gate(1)
        project_q(0)
        project_q(1)
    send_gate(1)

    @pl.when(core == 0)
    def _():
        passed(0)
        treat(3, 0)
        send_back(0)
        direct(1)
        treat(2, 1)
        send_back(1)
        passed(2)
        treat(2, 2, ends=True)
        pass

    @pl.when(core == 1)
    def _():
        direct(0)
        treat(3, 0)
        send_back(0)
        direct(2)
        treat(2, 2)
        send_back(1)
        passed(1)
        treat(2, 1, ends=True)
        pass

    with scope("pq2"):
        project_q(2)
    attend_at(2, [0])
    attend_at(0, [last])

    @pl.when(core == 0)
    def _():
        direct(3)
        treat(3, 3)
        passed(4)
        treat(3, 4)
        send_back(2)
        passed(5)
        treat(3, 5, ends=True)

    @pl.when(core == 1)
    def _():
        direct(4)
        treat(3, 4)
        direct(5)
        send_back(2)
        passed(3)
        treat(3, 3, 5, ends=True)

    for slot in range(seqs):
        if delayed(slot):

            @pl.when(s == last - 1)
            def _():
                kv_copy(slot, 0, rows, last).start()

    with scope("pq3"):
        project_q(3)
    attend_at(3, [0])
    attend_at(0, [last - 1])
    attend_at(1, [last - 1])
    send_back(3)
    attend_at(2, [last])
    attend_at(2, range(1, last))
    attend_at(0, range(last - 1))
    attend_at(1, range(last - 1))
    attend_at(3, range(1, spread))
    attend_at(1, [last])

    with scope("flush"):
        arrived(sent.at[pl.ds(1, seqs - 1)], out_recv.at[0])
    with scope("drain"):
        arrived(sent.at[pl.ds(1, seqs - 1)], out_send.at[0])
        arrived(off.at[pl.ds(1, seqs - 1)], off_send.at[0])
        arrived(tok.at[0], beside_send.at[0])
        for sender in range(2):
            many = sum(item[3] for item in crossings if item[0] == sender)

            @pl.when(core == sender)
            def _():
                for semaphore in (over_send, onward_send):
                    arrived(tok.at[pl.ds(0, 2), pl.ds(0, many // 2)], semaphore.at[0])

        def sent_to(target):
            arrived(gates.at[pl.ds(0, seqs), 0], gate_send.at[target])
            for source in range(target):
                skipped = sum(
                    target == last - 1 and source < returned(slot) for slot in range(seqs)
                )

                if skipped == seqs:
                    continue

                @pl.when(s == source)
                def _():
                    arrived(
                        kv.at[pl.ds(skipped, seqs - skipped), :, pl.ds(0, rows)],
                        kv_send.at[target],
                    )

        to_each(sent_to)

        @pl.when(s == last)
        def _():
            for slot in range(seqs):
                if returned(slot):
                    arrived(kv.at[slot, :, pl.ds(0, returned(slot) * rows)], back_send.at[slot])


def fused(
    tokens,
    forget_offset,
    q_weight,
    k_weight,
    v_weight,
    forget_weight,
    forget_bias,
    score_gain,
    out_gain,
):
    rows, width = tokens.shape[1:]
    head_count = forget_bias.shape[0]
    head_dim = out_gain.shape[0] // head_count
    seqs = lax.axis_size("dp")
    spread = lax.axis_size("sp")
    cols = q_weight.shape[1]
    heads = cols // head_dim
    padded = -(-heads // 8) * 8
    outside = pl.BlockSpec(memory_space=pltpu.HBM)
    dma = pltpu.SemaphoreType.DMA
    out = pl.pallas_call(
        fused_kernel,
        out_shape=pltpu.VMEM((rows, seqs * cols), jnp.bfloat16),
        in_specs=[outside] * 9,
        out_specs=pl.BlockSpec(memory_space=pltpu.VMEM),
        scratch_shapes=[
            pltpu.VMEM((seqs, rows, width), jnp.bfloat16),
            pltpu.VMEM((width, cols), jnp.bfloat16),
            pltpu.VMEM((width, 2 * head_dim), jnp.bfloat16),
            pltpu.VMEM((head_count, width), jnp.bfloat16),
            pltpu.VMEM((seqs, 1, rows), jnp.float32),
            pltpu.VMEM((1, head_count), jnp.float32),
            pltpu.SMEM((1, head_count), jnp.float32),
            pltpu.VMEM((1, head_count * head_dim), jnp.float32),
            pltpu.VMEM((seqs, heads * rows, head_dim), jnp.bfloat16),
            pltpu.VMEM((seqs, 2, spread * rows, head_dim), jnp.bfloat16),
            pltpu.VMEM((head_count, rows), jnp.float32),
            pltpu.VMEM((seqs, spread, padded, rows), jnp.float32),
            pltpu.VMEM((seqs, rows, cols), jnp.bfloat16),
            dma((9,)),
            pltpu.SemaphoreType.REGULAR((spread,)),
            dma((1,)),
            dma((1,)),
            dma((1,)),
            dma((2,)),
            dma((1,)),
            dma((6,)),
            dma((1,)),
            dma((6,)),
            dma((spread,)),
            dma((seqs,)),
            dma((spread,)),
            dma((seqs, spread)),
            dma((seqs,)),
            dma((1,)),
            dma((1,)),
        ],
        compiler_params=pltpu.CompilerParams(
            collective_id=0, has_side_effects=True
        ),
    )(
        tokens[0],
        forget_offset,
        q_weight,
        k_weight,
        v_weight,
        forget_weight.T,
        forget_bias[None, :],
        score_gain[None, :],
        out_gain[None, :],
    )
    return out[None]


def local(*args):
    tokens, k_weight, forget_bias, out_gain = args[0], args[3], args[6], args[8]
    head_dim = out_gain.shape[0] // forget_bias.shape[0]
    fits = tokens.shape[0] == 1 and tokens.shape[1] % 128 == 0 and head_dim % 128 == 0
    if (
        lax.axis_size("dp") == 4
        and 2 < lax.axis_size("sp") <= 4
        and k_weight.shape[1] == head_dim
        and fits
    ):
        return fused(*args)
    if k_weight.shape[1] % head_dim == 0 and tokens.shape[0] == 1:
        return heads_on_dp(*args)
    return heads_on_sp(*args)


def solution(mesh):
    in_specs = (
        P(("grp", "dp"), "sp", None),
        P(("grp", "dp"), "sp"),
        P(None, "dp"),
        P(None, "dp"),
        P(None, "dp"),
        P(),
        P(),
        P(),
        P(),
    )
    out_specs = P(("grp", "dp"), "sp", None)
    return jax.shard_map(local, mesh=mesh, in_specs=in_specs, out_specs=out_specs, check_vma=False)
```

```python
import functools

import jax
import jax.numpy as jnp
from jax import lax
from jax.experimental import pallas as pl
from jax.experimental.pallas import tpu as pltpu
from jax.sharding import PartitionSpec as P

NEG = -1e30
QK_FLOOR = 0.1
OUT_FLOOR = 0.001


def head_norm(vectors, floor):
    return vectors * lax.rsqrt(jnp.mean(vectors * vectors, axis=-1, keepdims=True) + floor)


def heads_on_sp(
    tokens,
    forget_offset,
    q_weight,
    k_weight,
    v_weight,
    forget_weight,
    forget_bias,
    score_gain,
    out_gain,
):
    own_rows = tokens[0]
    tok_count = own_rows.shape[0]
    head_count = forget_bias.shape[0]
    head_dim = out_gain.shape[0] // head_count
    kv_heads = k_weight.shape[1] * lax.axis_size("dp") // head_dim
    spread = lax.axis_size("sp")
    local_heads = head_count // spread
    local_kv = max(1, kv_heads // spread)
    group_size = local_heads // local_kv
    everyone = lax.all_gather(tokens, "dp", axis=0, tiled=True)
    seq_count = everyone.shape[0]
    flat_rows = everyone.reshape(seq_count * tok_count, everyone.shape[2])
    query_cols = (
        jnp.dot(flat_rows, q_weight, preferred_element_type=jnp.float32)
        .astype(jnp.bfloat16)
        .reshape(seq_count, tok_count, -1)
    )
    key_cols = (
        jnp.dot(flat_rows, k_weight, preferred_element_type=jnp.float32)
        .astype(jnp.bfloat16)
        .reshape(seq_count, tok_count, -1)
    )
    value_cols = (
        jnp.dot(flat_rows, v_weight, preferred_element_type=jnp.float32)
        .astype(jnp.bfloat16)
        .reshape(seq_count, tok_count, -1)
    )
    query_mine, key_mine, value_mine = (
        lax.all_to_all(query_cols, "dp", split_axis=0, concat_axis=2, tiled=True),
        lax.all_to_all(key_cols, "dp", split_axis=0, concat_axis=2, tiled=True),
        lax.all_to_all(value_cols, "dp", split_axis=0, concat_axis=2, tiled=True),
    )
    queries = query_mine[0]
    keys_proj = key_mine[0]
    values_proj = value_mine[0]
    forget_input = (
        jnp.dot(own_rows, forget_weight, preferred_element_type=jnp.float32)
        + forget_offset[0][:, None]
    ).astype(jnp.bfloat16)
    query_send = queries.reshape(tok_count, spread, local_heads, head_dim)
    forget_send = forget_input.reshape(tok_count, spread, local_heads)
    if kv_heads >= spread:
        key_send = keys_proj.reshape(tok_count, spread, local_kv, head_dim)
        value_send = values_proj.reshape(tok_count, spread, local_kv, head_dim)
    else:
        copies = spread // kv_heads
        key_send = jnp.broadcast_to(
            keys_proj.reshape(tok_count, kv_heads, 1, head_dim),
            (tok_count, kv_heads, copies, head_dim),
        ).reshape(tok_count, spread, 1, head_dim)
        value_send = jnp.broadcast_to(
            values_proj.reshape(tok_count, kv_heads, 1, head_dim),
            (tok_count, kv_heads, copies, head_dim),
        ).reshape(tok_count, spread, 1, head_dim)
    query_head, forget_head, key_head, value_head = (
        lax.all_to_all(query_send, "sp", split_axis=1, concat_axis=0, tiled=True),
        lax.all_to_all(forget_send, "sp", split_axis=1, concat_axis=0, tiled=True),
        lax.all_to_all(key_send, "sp", split_axis=1, concat_axis=0, tiled=True),
        lax.all_to_all(value_send, "sp", split_axis=1, concat_axis=0, tiled=True),
    )
    length = query_head.shape[0]
    first_head = lax.axis_index("sp") * local_heads
    bias_local = lax.dynamic_slice_in_dim(forget_bias, first_head, local_heads, 0)
    gain_local = lax.dynamic_slice_in_dim(score_gain, first_head, local_heads, 0)
    norm_local = lax.dynamic_slice_in_dim(
        out_gain, first_head * head_dim, local_heads * head_dim, 0
    )
    log_gate = jax.nn.log_sigmoid(
        forget_head.reshape(length, local_heads).astype(jnp.float32) + bias_local[None, :]
    )
    cumulative = jnp.cumsum(log_gate, axis=0).reshape(length, local_kv, group_size)
    query_unit = head_norm(query_head.astype(jnp.float32), QK_FLOOR).astype(jnp.bfloat16)
    key_unit = head_norm(
        key_head.reshape(length, local_kv, head_dim).astype(jnp.float32), QK_FLOOR
    ).astype(jnp.bfloat16)
    value_heads = value_head.reshape(length, local_kv, head_dim)
    factor = (gain_local * head_dim ** (-0.5)).reshape(local_kv, group_size)
    out_gains = norm_local.reshape(local_kv, group_size, head_dim)
    key_totals = jnp.transpose(cumulative, (1, 2, 0))
    span_rows = 512
    positions = jnp.arange(length, dtype=jnp.int32)

    def attend_block(block_index):
        first = block_index * span_rows
        query_block = lax.dynamic_slice_in_dim(query_unit, first, span_rows, 0)
        query_totals = lax.dynamic_slice_in_dim(cumulative, first, span_rows, 0)
        scores = jnp.einsum(
            "qkgd,skd->kgqs", query_block, key_unit, preferred_element_type=jnp.float32
        )
        scores = (
            scores * factor[:, :, None, None]
            + jnp.transpose(query_totals, (1, 2, 0))[..., None]
            - key_totals[:, :, None, :]
        )
        allowed = positions[None, :] <= (first + jnp.arange(span_rows, dtype=jnp.int32))[:, None]
        scores = jnp.where(allowed[None, None], scores, NEG)
        row_peak = jnp.max(scores, axis=-1, keepdims=True)
        exponent = jnp.exp(scores - row_peak)
        weights = (exponent / jnp.sum(exponent, axis=-1, keepdims=True)).astype(jnp.bfloat16)
        mixed = jnp.einsum(
            "kgqs,skd->qkgd", weights, value_heads, preferred_element_type=jnp.float32
        )
        return (head_norm(mixed, OUT_FLOOR) * out_gains).astype(jnp.bfloat16)

    outputs = lax.map(attend_block, jnp.arange(length // span_rows, dtype=jnp.int32))
    outputs = outputs.reshape(length, local_heads, head_dim)
    back_rows = lax.all_to_all(outputs, "sp", split_axis=0, concat_axis=1, tiled=True)
    return back_rows.reshape(1, tok_count, head_count * head_dim)


def heads_on_dp(
    tokens,
    forget_offset,
    q_weight,
    k_weight,
    v_weight,
    forget_weight,
    forget_bias,
    score_gain,
    out_gain,
):
    tok_count = tokens.shape[1]
    head_count = forget_bias.shape[0]
    head_dim = out_gain.shape[0] // head_count
    seq_count = lax.axis_size("dp")
    kv = k_weight.shape[1] // head_dim
    heads = q_weight.shape[1] // head_dim
    group = heads // kv
    everyone = lax.all_gather(tokens, "dp", axis=0, tiled=True)
    offsets = lax.all_gather(forget_offset, "dp", axis=0, tiled=True)
    flat = everyone.reshape(seq_count * tok_count, -1)
    first = lax.axis_index("dp") * heads

    def mine(array):
        return lax.dynamic_slice_in_dim(array, first, heads, array.ndim - 1)

    def project(weight):
        return jnp.dot(flat, weight, preferred_element_type=jnp.float32).astype(jnp.bfloat16)

    key_unit = head_norm(
        project(k_weight).astype(jnp.float32).reshape(seq_count, tok_count, kv, head_dim), QK_FLOOR
    ).astype(jnp.bfloat16)
    values = project(v_weight).reshape(seq_count, tok_count, kv, head_dim)
    pair = lax.all_gather(jnp.stack([key_unit, values]), "sp", axis=2, tiled=True)
    forget_input = (
        jnp.dot(flat, mine(forget_weight), preferred_element_type=jnp.float32)
        + offsets.reshape(-1)[:, None]
    ).astype(jnp.bfloat16)
    log_gate = jax.nn.log_sigmoid(forget_input.astype(jnp.float32) + mine(forget_bias)[None, :])
    gates = lax.all_gather(
        log_gate.reshape(seq_count, tok_count, heads), "sp", axis=1, tiled=True
    )
    cumulative = jnp.cumsum(gates, axis=1)
    length = gates.shape[1]
    start = lax.axis_index("sp") * tok_count
    own = lax.dynamic_slice_in_dim(cumulative, start, tok_count, 1)
    query_unit = head_norm(
        project(q_weight).astype(jnp.float32).reshape(seq_count, tok_count, kv, group, head_dim),
        QK_FLOOR,
    ).astype(jnp.bfloat16)
    factor = (mine(score_gain) * head_dim ** (-0.5)).reshape(kv, group)
    scores = jnp.einsum(
        "bqkgd,bskd->bkgqs", query_unit, pair[0], preferred_element_type=jnp.float32
    )
    by_head = jnp.transpose(own.reshape(seq_count, tok_count, kv, group), (0, 2, 3, 1))
    by_key = jnp.transpose(cumulative.reshape(seq_count, length, kv, group), (0, 2, 3, 1))
    scores = (
        scores * factor[None, :, :, None, None] + by_head[..., None] - by_key[..., None, :]
    )
    allowed = jnp.arange(length)[None, :] <= (start + jnp.arange(tok_count))[:, None]
    scores = jnp.where(allowed, scores, NEG)
    exponent = jnp.exp(scores - jnp.max(scores, axis=-1, keepdims=True))
    weights = (exponent / jnp.sum(exponent, axis=-1, keepdims=True)).astype(jnp.bfloat16)
    mixed = jnp.einsum(
        "bkgqs,bskd->bqkgd", weights, pair[1], preferred_element_type=jnp.float32
    )
    gains = lax.dynamic_slice_in_dim(out_gain, first * head_dim, heads * head_dim, 0)
    outputs = (head_norm(mixed, OUT_FLOOR) * gains.reshape(kv, group, head_dim)).astype(
        jnp.bfloat16
    )
    outputs = outputs.reshape(seq_count, tok_count, heads * head_dim)
    return lax.all_to_all(outputs, "dp", split_axis=0, concat_axis=2, tiled=True)


LOG2E = 1.4426950408889634


def fused_kernel(
    tok_in,
    off_in,
    qw_in,
    kw_in,
    vw_in,
    fw_in,
    bias_in,
    gain_in,
    norm_in,
    result,
    tok,
    qw,
    kvw,
    fw,
    off,
    bias_row,
    gain,
    norm,
    q_unit,
    kv,
    running_all,
    gates,
    sent,
    load_sem,
    ready,
    off_send,
    off_recv,
    beside_send,
    beside_recv,
    over_send,
    cross_recv,
    onward_send,
    gate_send,
    gate_recv,
    kv_send,
    kv_recv,
    back_send,
    out_send,
    out_recv,
):
    d = lax.axis_index("dp")
    s = lax.axis_index("sp")
    spread = lax.axis_size("sp")
    rows, width = tok_in.shape
    half, quarter = rows // 2, rows // 4
    cols = qw_in.shape[1]
    head_dim = kw_in.shape[1]
    heads = cols // head_dim
    seqs = tok.shape[0]
    chip, core = d // 2, d % 2
    last = spread - 1
    scope = jax.named_scope

    def peer(step):
        across = step // 2
        own_chip = (1 - across) * ((core + step % 2) % 2)
        return ((chip + across) % 2) * 2 + across * (step % 2) + own_chip

    def seen_as(step):
        return (step // 2) * (2 + core) + (1 - step // 2) * step

    def remote(src, dst, send, recv, **target):
        return pltpu.make_async_remote_copy(
            src_ref=src,
            dst_ref=dst,
            send_sem=send,
            recv_sem=recv,
            device_id=target,
            device_id_type=pl.DeviceIdType.MESH,
        )

    barrier = pltpu.get_barrier_semaphore()
    for step in range(1, seqs):
        pl.semaphore_signal(
            barrier, inc=1, device_id={"dp": peer(step)}, device_id_type=pl.DeviceIdType.MESH
        )

    @pl.when(s > 0)
    def _():
        pl.semaphore_signal(
            barrier, inc=1, device_id={"sp": s - 1}, device_id_type=pl.DeviceIdType.MESH
        )

    @pl.when(s < last)
    def _():
        pl.semaphore_signal(
            barrier, inc=1, device_id={"sp": s + 1}, device_id_type=pl.DeviceIdType.MESH
        )

    def load(src, dst, index):
        copy = pltpu.make_async_copy(src, dst, load_sem.at[index])
        copy.start()
        return copy

    load_tok = load(tok_in, tok.at[0], 0)
    load_off = load(off_in, off.at[0], 1)
    load_k = load(kw_in, kvw.at[:, pl.ds(0, head_dim)], 2)
    load_v = load(vw_in, kvw.at[:, pl.ds(head_dim, head_dim)], 3)
    load_f = load(fw_in, fw, 4)
    load_b = load(bias_in, bias_row, 5)
    load_g = load(gain_in, gain, 6)
    load_n = load(norm_in, norm, 7)
    load_q = load(qw_in, qw, 8)

    load_tok.wait()
    load_off.wait()
    with scope("bar"):
        pl.semaphore_wait(barrier, seqs - 1 + (s + last) // spread + 1 - (s + 1) // spread)

    def tell_back(target):
        pl.semaphore_signal(
            ready.at[target], inc=1, device_id={"sp": s - 1}, device_id_type=pl.DeviceIdType.MESH
        )

    @pl.when(jnp.logical_and(s > 0, s < last))
    def _():
        tell_back(s + 1)

    def await_ready(source):
        for target in range(source + 2, spread):
            pl.semaphore_wait(ready.at[target], 1)
            if source > 0:
                tell_back(target)

    offs = [
        remote(off.at[0], off.at[seen_as(step)], off_send.at[0], off_recv.at[0], dp=peer(step))
        for step in range(1, seqs)
    ]
    for copy in offs:
        copy.start()

    def half_of(index):
        return pl.ds(pl.multiple_of(index * half, half), half)

    beside = [
        remote(
            tok.at[0, half_of(part)], tok.at[1, half_of(part)], beside_send.at[0],
            beside_recv.at[i], dp=peer(1),
        )
        for i, part in enumerate((1 - core, core))
    ]
    crossings = [
        (1, 3, 0, quarter),
        (0, 2, 0, half),
        (1, 2, half, half),
        (0, 3, quarter, quarter),
        (1, 3, half, quarter),
        (1, 3, half + quarter, quarter),
    ]
    over, onward = [], []
    for j, (sender, slot, first, count) in enumerate(crossings):
        part = pl.ds(first, count)
        held = 0 if sender == slot - 2 else 1
        over.append(
            remote(
                tok.at[held, part], tok.at[slot, part], over_send.at[0], cross_recv.at[j],
                dp=(1 - chip) * 2 + core,
            )
        )
        onward.append(
            remote(
                tok.at[slot, part], tok.at[slot, part], onward_send.at[0], cross_recv.at[j],
                dp=peer(1),
            )
        )

    @pl.when(core == 0)
    def _():
        over[1].start()

    @pl.when(core == 1)
    def _():
        over[0].start()

    for copy in beside:
        copy.start()

    def unit(vectors):
        vectors = vectors.astype(jnp.bfloat16).astype(jnp.float32)
        return head_norm(vectors, QK_FLOOR).astype(jnp.bfloat16)

    def returned(slot):
        return (last - 1, last - 1, 1, 1)[slot]

    def delayed(slot):
        return slot == 1

    def to_each(act):
        for target in range(last, 0, -1):

            @pl.when(s < target)
            def _():
                act(target)

    def halved(slot, block):
        return slot > 1 and block == 0

    def parts_of(slot, late):
        if slot < 2:
            return [(0, rows)]
        return [(pl.multiple_of((late + core - 2 * late * core) * half, half), half)]

    final = seqs - 1
    final_parts = {
        (0, 0): [(0, half + quarter)],
        (0, 1): [(half + quarter, quarter)],
        (1, 0): [(0, quarter), (half, quarter)],
        (1, 1): [(quarter, quarter), (half + quarter, quarter)],
    }

    def final_rows(c, late):
        return sum(count for _, count in final_parts[c, late])

    def on_core(act):
        for c in range(2):

            @pl.when(core == c)
            def _():
                act(c)

    def await_final(late):
        def act(c):
            group = kv_recv.at[final, last if late else 0]
            arrived(kv.at[final, :, pl.ds(0, final_rows(c, late))], group)

        on_core(act)

    def kv_copy(slot, first, count, target, late=False):
        piece = kv.at[slot, :, pl.ds(pl.multiple_of(s * rows + first, quarter), count)]
        group = s + late * (last - last * ((s + last) // spread))
        return remote(piece, piece, kv_send.at[target], kv_recv.at[slot, group], sp=target)

    def gate_copy(slot, target):
        piece = gates.at[slot, s]
        return remote(piece, piece, gate_send.at[target], gate_recv.at[slot], sp=target)

    def back_copy(slot, block, first, count, late):
        piece = kv.at[slot, :, pl.ds(block * rows + first, count)]
        group = last if late else block
        return remote(piece, piece, back_send.at[slot], kv_recv.at[slot, group], sp=last - 1)

    def send_kv(slot, *parts, late=False, straight=False):
        def act(target):
            skip_from = last - 1 if target == last and delayed(slot) else last
            for first, count in parts:
                skip_below = returned(slot) if target == last - 1 and not straight else 0

                @pl.when(jnp.logical_and(s >= skip_below, s < skip_from))
                def _():
                    kv_copy(slot, first, count, target, late).start()

        to_each(act)

    def send_gate(slot):
        to_each(lambda target: gate_copy(slot, target).start())

    def project_kv(slot, *parts):
        pair = jnp.dot(
            jnp.concatenate([tok[slot, first : first + count] for first, count in parts], axis=0),
            kvw[...],
            preferred_element_type=jnp.float32,
        )
        done = 0
        for first, count in parts:
            here = pl.ds(pl.multiple_of(s * rows + first, quarter), count)
            piece = pair[done : done + count]
            kv[slot, 0, here] = unit(piece[:, :head_dim])
            kv[slot, 1, here] = piece[:, head_dim:].astype(jnp.bfloat16)
            done += count

    def project_q(slot):
        queries = jnp.dot(tok[slot], qw[...], preferred_element_type=jnp.float32)
        for h in range(heads):
            q_unit[slot, pl.ds(h * rows, rows)] = unit(
                queries[:, h * head_dim : (h + 1) * head_dim]
            )

    count = bias_in.shape[1]

    def gate(slot):
        forget_input = (
            lax.dot_general(
                fw[...], tok[slot], (((1,), (1,)), ((), ())), preferred_element_type=jnp.float32
            )
            + off[slot]
        ).astype(jnp.bfloat16)
        square = (count, count)
        diagonal = lax.broadcasted_iota(jnp.int32, square, 0) == lax.broadcasted_iota(
            jnp.int32, square, 1
        )
        bias = jnp.sum(
            jnp.where(diagonal, jnp.broadcast_to(bias_row[...], square), 0.0),
            axis=1,
            keepdims=True,
        )
        gate_arg = forget_input.astype(jnp.float32) + bias
        log_gate = jnp.minimum(gate_arg, 0.0) - jnp.log1p(jnp.exp(-jnp.abs(gate_arg)))
        before = lax.broadcasted_iota(jnp.int32, (rows, rows), 0)
        after = lax.broadcasted_iota(jnp.int32, (rows, rows), 1)
        upto = (before <= after).astype(jnp.bfloat16)
        high = log_gate.astype(jnp.bfloat16)
        rest = log_gate - high.astype(jnp.float32)
        middle = rest.astype(jnp.bfloat16)
        low = (rest - middle.astype(jnp.float32)).astype(jnp.bfloat16)
        running = (
            jnp.dot(low, upto, preferred_element_type=jnp.float32)
            + jnp.dot(middle, upto, preferred_element_type=jnp.float32)
            + jnp.dot(high, upto, preferred_element_type=jnp.float32)
        )
        running_all[...] = running * LOG2E
        own = running_all[pl.ds(d * heads, heads)]
        spare = gates.shape[2] - heads
        if spare:
            own = jnp.concatenate([own, jnp.zeros((spare, rows), jnp.float32)], axis=0)
        gates[slot, s] = own

    def out_copy(slot, start, group):
        place = pl.ds(
            pl.multiple_of(d * cols + start * head_dim, head_dim), group * head_dim
        )
        return remote(
            sent.at[slot, :, pl.ds(start * head_dim, group * head_dim)], result.at[:, place],
            out_send.at[0], out_recv.at[0], dp=peer(slot),
        )

    def attend(slot, blocks, groups):
        span = blocks * rows
        later = jnp.zeros((gates.shape[2], 1), jnp.float32)
        totals = [gates[slot, blocks - 1]]
        for b in range(blocks - 2, -1, -1):
            local_sum = gates[slot, b]
            later = later + local_sum[:, rows - 1 :]
            totals.insert(0, local_sum - later)
        allowed = lax.broadcasted_iota(jnp.int32, (rows, rows), 1) <= lax.broadcasted_iota(
            jnp.int32, (rows, rows), 0
        )
        keys = kv[slot, 0, :span]
        values = kv[slot, 1, :span]
        start = 0
        for group in groups:
            each = range(start, start + group)
            raw = [
                lax.dot_general(
                    q_unit[slot, pl.ds(h * rows, rows)],
                    keys,
                    (((1,), (1,)), ((), ())),
                    preferred_element_type=jnp.float32,
                )
                for h in each
            ]
            scores = []
            for h, product in zip(each, raw):
                factor = gain[0, d * heads + h] * (head_dim ** (-0.5) * LOG2E)
                parts = [
                    product[:, b * rows : (b + 1) * rows] * factor - totals[b][h : h + 1, :]
                    for b in range(blocks)
                ]
                parts[-1] = jnp.where(allowed, parts[-1], NEG)
                scores.append(parts)
            peaks = [
                jnp.max(functools.reduce(jnp.maximum, parts), axis=-1, keepdims=True)
                for parts in scores
            ]
            exponents = [
                [jnp.exp2(part - peak) for part in parts] for parts, peak in zip(scores, peaks)
            ]
            scales = [
                1.0 / jnp.sum(functools.reduce(jnp.add, parts), axis=-1, keepdims=True)
                for parts in exponents
            ]
            weights = [
                jnp.concatenate([(part * scale).astype(jnp.bfloat16) for part in parts], axis=1)
                for parts, scale in zip(exponents, scales)
            ]
            mixed = [jnp.dot(w, values, preferred_element_type=jnp.float32) for w in weights]
            for h, rough in zip(each, mixed):
                place = pl.ds(pl.multiple_of(d * cols + h * head_dim, head_dim), head_dim)
                outcome = (head_norm(rough, OUT_FLOOR) * norm[:, place]).astype(jnp.bfloat16)
                if slot == 0:
                    result[:, place] = outcome
                else:
                    sent[slot, :, h * head_dim : (h + 1) * head_dim] = outcome
            if slot > 0:
                out_copy(slot, start, group).start()
            start += group

    in_turn = [1] * (heads // 2) + [heads - heads // 2]

    def arrived(ref, semaphore):
        pltpu.make_async_copy(ref, ref, semaphore).wait()

    def await_kv(slot, blocks):
        for b in blocks:
            if halved(slot, b) and slot == final:
                await_final(0)
                await_final(1)
            elif halved(slot, b):
                arrived(kv.at[slot, :, pl.ds(b * rows, half)], kv_recv.at[slot, b])
                arrived(kv.at[slot, :, pl.ds(b * rows, half)], kv_recv.at[slot, last])
            else:
                arrived(kv.at[slot, :, pl.ds(b * rows, rows)], kv_recv.at[slot, b])

    def send_back(slot, late=0):
        @pl.when(s == last)
        def _():
            with scope(f"bk{slot}{late}"):
                if slot == final:
                    await_final(late)
                elif slot > 1:
                    group = kv_recv.at[slot, last if late else 0]
                    arrived(kv.at[slot, :, pl.ds(0, half)], group)
                else:
                    await_kv(slot, range(returned(slot)))
            if slot == final:

                def act(c):
                    if (c, late) != (0, 1):
                        for first, count in final_parts[c, late]:
                            back_copy(slot, 0, first, count, late).start()

                on_core(act)
            else:
                for b in range(returned(slot)):
                    for first, count in parts_of(slot, late):
                        back_copy(slot, b, first, count, late).start()

    def attend_at(slot, places):
        for k in places:

            @pl.when(s == k)
            def _():
                if k > 0:
                    with scope(f"wkv{slot}"):
                        arrived(gates.at[slot, pl.ds(0, k)], gate_recv.at[slot])
                        await_kv(slot, range(returned(slot) if k == last else 0, k))
                with scope(f"att{slot}"):
                    attend(slot, k + 1, in_turn if slot == seqs - 1 else [heads])

    def direct(j):
        with scope(f"wx{j}"):
            over[j].wait_recv()
        onward[j].start()

    def passed(j):
        with scope(f"wo{j}"):
            onward[j].wait_recv()

    def whole(j):
        return crossings[j][2:]

    def treat(slot, *js, ends=False, late=False, straight=False):
        parts = [whole(j) for j in js]
        with scope(f"p{slot}" + "".join(map(str, js))):
            project_kv(slot, *parts)
            if ends:
                gate(slot)
        if ends:
            send_gate(slot)
        send_kv(slot, *parts, late=late, straight=straight)

    load_k.wait()
    load_v.wait()
    with scope("pkv0"):
        project_kv(0, (0, rows))
    for source in range(1, spread - 1):

        @pl.when(s == source)
        def _():
            await_ready(source)

    @pl.when(s > 0)
    def _():
        send_kv(0, (0, rows))

    with scope("wb0"):
        beside[0].wait_recv()

    @pl.when(core == 0)
    def _():
        over[3].start()

    @pl.when(core == 1)
    def _():
        over[2].start()
        over[4].start()
        over[5].start()

    load_f.wait()
    load_b.wait()
    with scope("wb1"):
        beside[1].wait_recv()
    with scope("pkv1g0"):
        gate(0)
        project_kv(1, (0, rows))

    @pl.when(s == 0)
    def _():
        with scope("rdy"):
            await_ready(0)
        send_kv(0, (0, rows))

    send_gate(0)
    send_kv(1, (0, rows))
    load_q.wait()
    load_g.wait()
    load_n.wait()
    with scope("woff"):
        arrived(off.at[pl.ds(1, seqs - 1)], off_recv.at[0])
    with scope("pq01g1"):
        gate(1)
        project_q(0)
        project_q(1)
    send_gate(1)

    @pl.when(core == 0)
    def _():
        passed(0)
        treat(3, 0)
        send_back(0)
        direct(1)
        treat(2, 1)
        send_back(1)
        passed(2)
        treat(2, 2, ends=True, late=True)

    @pl.when(core == 1)
    def _():
        direct(0)
        treat(3, 0)
        send_back(0)
        direct(2)
        treat(2, 2)
        send_back(1)
        passed(1)
        treat(2, 1, ends=True, late=True)

    with scope("pq2"):
        project_q(2)
    send_back(2)
    attend_at(0, [last])

    @pl.when(core == 0)
    def _():
        direct(3)
        treat(3, 3)
        passed(4)
        treat(3, 4)
        send_back(2, 1)
        passed(5)
        treat(3, 5, ends=True, late=True, straight=True)

    @pl.when(core == 1)
    def _():
        direct(4)
        treat(3, 4)
        direct(5)
        send_back(2, 1)
        passed(3)
        treat(3, 3, 5, ends=True, late=True)

    for slot in range(seqs):
        if delayed(slot):

            @pl.when(s == last - 1)
            def _():
                kv_copy(slot, 0, rows, last).start()

    with scope("pq3"):
        project_q(3)
    attend_at(2, [0])
    attend_at(3, [0])
    attend_at(0, [last - 1])
    attend_at(1, [last - 1])
    send_back(3)
    send_back(3, 1)
    attend_at(2, [last])
    attend_at(2, range(1, last))
    attend_at(0, range(last - 1))
    attend_at(1, range(last - 1))
    attend_at(3, range(1, spread))
    attend_at(1, [last])

    with scope("flush"):
        arrived(sent.at[pl.ds(1, seqs - 1)], out_recv.at[0])
    with scope("drain"):
        arrived(sent.at[pl.ds(1, seqs - 1)], out_send.at[0])
        arrived(off.at[pl.ds(1, seqs - 1)], off_send.at[0])
        arrived(tok.at[0], beside_send.at[0])
        for sender in range(2):
            many = sum(item[3] for item in crossings if item[0] == sender)

            @pl.when(core == sender)
            def _():
                for semaphore in (over_send, onward_send):
                    arrived(tok.at[pl.ds(0, 2), pl.ds(0, many // 2)], semaphore.at[0])

        def sent_to(target):
            arrived(gates.at[pl.ds(0, seqs), 0], gate_send.at[target])
            for source in range(target):
                skipped = sum(
                    target == last - 1 and source < returned(slot) for slot in range(seqs)
                )
                if skipped == seqs:

                    @pl.when(jnp.logical_and(s == source, core == 0))
                    def _():
                        arrived(
                            kv.at[final, :, pl.ds(0, final_rows(0, 1))], kv_send.at[target]
                        )

                    continue

                @pl.when(s == source)
                def _():
                    arrived(
                        kv.at[pl.ds(skipped, seqs - skipped), :, pl.ds(0, rows)],
                        kv_send.at[target],
                    )

        to_each(sent_to)

        @pl.when(s == last)
        def _():
            for slot in range(seqs):
                if slot < final:
                    arrived(kv.at[slot, :, pl.ds(0, returned(slot) * rows)], back_send.at[slot])

            def act(c):
                many = rows if c else final_rows(0, 0)
                arrived(kv.at[final, :, pl.ds(0, many)], back_send.at[final])

            on_core(act)


def fused(
    tokens,
    forget_offset,
    q_weight,
    k_weight,
    v_weight,
    forget_weight,
    forget_bias,
    score_gain,
    out_gain,
):
    rows, width = tokens.shape[1:]
    head_count = forget_bias.shape[0]
    head_dim = out_gain.shape[0] // head_count
    seqs = lax.axis_size("dp")
    spread = lax.axis_size("sp")
    cols = q_weight.shape[1]
    heads = cols // head_dim
    padded = -(-heads // 8) * 8
    outside = pl.BlockSpec(memory_space=pltpu.HBM)
    dma = pltpu.SemaphoreType.DMA
    out = pl.pallas_call(
        fused_kernel,
        out_shape=pltpu.VMEM((rows, seqs * cols), jnp.bfloat16),
        in_specs=[outside] * 9,
        out_specs=pl.BlockSpec(memory_space=pltpu.VMEM),
        scratch_shapes=[
            pltpu.VMEM((seqs, rows, width), jnp.bfloat16),
            pltpu.VMEM((width, cols), jnp.bfloat16),
            pltpu.VMEM((width, 2 * head_dim), jnp.bfloat16),
            pltpu.VMEM((head_count, width), jnp.bfloat16),
            pltpu.VMEM((seqs, 1, rows), jnp.float32),
            pltpu.VMEM((1, head_count), jnp.float32),
            pltpu.SMEM((1, head_count), jnp.float32),
            pltpu.VMEM((1, head_count * head_dim), jnp.float32),
            pltpu.VMEM((seqs, heads * rows, head_dim), jnp.bfloat16),
            pltpu.VMEM((seqs, 2, spread * rows, head_dim), jnp.bfloat16),
            pltpu.VMEM((head_count, rows), jnp.float32),
            pltpu.VMEM((seqs, spread, padded, rows), jnp.float32),
            pltpu.VMEM((seqs, rows, cols), jnp.bfloat16),
            dma((9,)),
            pltpu.SemaphoreType.REGULAR((spread,)),
            dma((1,)),
            dma((1,)),
            dma((1,)),
            dma((2,)),
            dma((1,)),
            dma((6,)),
            dma((1,)),
            dma((spread,)),
            dma((seqs,)),
            dma((spread,)),
            dma((seqs, spread)),
            dma((seqs,)),
            dma((1,)),
            dma((1,)),
        ],
        compiler_params=pltpu.CompilerParams(
            collective_id=0, has_side_effects=True
        ),
    )(
        tokens[0],
        forget_offset,
        q_weight,
        k_weight,
        v_weight,
        forget_weight.T,
        forget_bias[None, :],
        score_gain[None, :],
        out_gain[None, :],
    )
    return out[None]


def local(*args):
    tokens, k_weight, forget_bias, out_gain = args[0], args[3], args[6], args[8]
    head_dim = out_gain.shape[0] // forget_bias.shape[0]
    fits = tokens.shape[0] == 1 and tokens.shape[1] % 128 == 0 and head_dim % 128 == 0
    if (
        lax.axis_size("dp") == 4
        and 2 < lax.axis_size("sp") <= 4
        and k_weight.shape[1] == head_dim
        and fits
    ):
        return fused(*args)
    if k_weight.shape[1] % head_dim == 0 and tokens.shape[0] == 1:
        return heads_on_dp(*args)
    return heads_on_sp(*args)


def solution(mesh):
    in_specs = (
        P(("grp", "dp"), "sp", None),
        P(("grp", "dp"), "sp"),
        P(None, "dp"),
        P(None, "dp"),
        P(None, "dp"),
        P(),
        P(),
        P(),
        P(),
    )
    out_specs = P(("grp", "dp"), "sp", None)
    return jax.shard_map(local, mesh=mesh, in_specs=in_specs, out_specs=out_specs, check_vma=False)
```

```python
import functools

import jax
import jax.numpy as jnp
from jax import lax
from jax.experimental import pallas as pl
from jax.experimental.pallas import tpu as pltpu
from jax.sharding import PartitionSpec as P

NEG = -1e30
QK_FLOOR = 0.1
OUT_FLOOR = 0.001


def head_norm(vectors, floor):
    return vectors * lax.rsqrt(jnp.mean(vectors * vectors, axis=-1, keepdims=True) + floor)


def heads_on_sp(
    tokens,
    forget_offset,
    q_weight,
    k_weight,
    v_weight,
    forget_weight,
    forget_bias,
    score_gain,
    out_gain,
):
    own_rows = tokens[0]
    tok_count = own_rows.shape[0]
    head_count = forget_bias.shape[0]
    head_dim = out_gain.shape[0] // head_count
    kv_heads = k_weight.shape[1] * lax.axis_size("dp") // head_dim
    spread = lax.axis_size("sp")
    local_heads = head_count // spread
    local_kv = max(1, kv_heads // spread)
    group_size = local_heads // local_kv
    everyone = lax.all_gather(tokens, "dp", axis=0, tiled=True)
    seq_count = everyone.shape[0]
    flat_rows = everyone.reshape(seq_count * tok_count, everyone.shape[2])
    query_cols = (
        jnp.dot(flat_rows, q_weight, preferred_element_type=jnp.float32)
        .astype(jnp.bfloat16)
        .reshape(seq_count, tok_count, -1)
    )
    key_cols = (
        jnp.dot(flat_rows, k_weight, preferred_element_type=jnp.float32)
        .astype(jnp.bfloat16)
        .reshape(seq_count, tok_count, -1)
    )
    value_cols = (
        jnp.dot(flat_rows, v_weight, preferred_element_type=jnp.float32)
        .astype(jnp.bfloat16)
        .reshape(seq_count, tok_count, -1)
    )
    query_mine, key_mine, value_mine = (
        lax.all_to_all(query_cols, "dp", split_axis=0, concat_axis=2, tiled=True),
        lax.all_to_all(key_cols, "dp", split_axis=0, concat_axis=2, tiled=True),
        lax.all_to_all(value_cols, "dp", split_axis=0, concat_axis=2, tiled=True),
    )
    queries = query_mine[0]
    keys_proj = key_mine[0]
    values_proj = value_mine[0]
    forget_input = (
        jnp.dot(own_rows, forget_weight, preferred_element_type=jnp.float32)
        + forget_offset[0][:, None]
    ).astype(jnp.bfloat16)
    query_send = queries.reshape(tok_count, spread, local_heads, head_dim)
    forget_send = forget_input.reshape(tok_count, spread, local_heads)
    if kv_heads >= spread:
        key_send = keys_proj.reshape(tok_count, spread, local_kv, head_dim)
        value_send = values_proj.reshape(tok_count, spread, local_kv, head_dim)
    else:
        copies = spread // kv_heads
        key_send = jnp.broadcast_to(
            keys_proj.reshape(tok_count, kv_heads, 1, head_dim),
            (tok_count, kv_heads, copies, head_dim),
        ).reshape(tok_count, spread, 1, head_dim)
        value_send = jnp.broadcast_to(
            values_proj.reshape(tok_count, kv_heads, 1, head_dim),
            (tok_count, kv_heads, copies, head_dim),
        ).reshape(tok_count, spread, 1, head_dim)
    query_head, forget_head, key_head, value_head = (
        lax.all_to_all(query_send, "sp", split_axis=1, concat_axis=0, tiled=True),
        lax.all_to_all(forget_send, "sp", split_axis=1, concat_axis=0, tiled=True),
        lax.all_to_all(key_send, "sp", split_axis=1, concat_axis=0, tiled=True),
        lax.all_to_all(value_send, "sp", split_axis=1, concat_axis=0, tiled=True),
    )
    length = query_head.shape[0]
    first_head = lax.axis_index("sp") * local_heads
    bias_local = lax.dynamic_slice_in_dim(forget_bias, first_head, local_heads, 0)
    gain_local = lax.dynamic_slice_in_dim(score_gain, first_head, local_heads, 0)
    norm_local = lax.dynamic_slice_in_dim(
        out_gain, first_head * head_dim, local_heads * head_dim, 0
    )
    log_gate = jax.nn.log_sigmoid(
        forget_head.reshape(length, local_heads).astype(jnp.float32) + bias_local[None, :]
    )
    cumulative = jnp.cumsum(log_gate, axis=0).reshape(length, local_kv, group_size)
    query_unit = head_norm(query_head.astype(jnp.float32), QK_FLOOR).astype(jnp.bfloat16)
    key_unit = head_norm(
        key_head.reshape(length, local_kv, head_dim).astype(jnp.float32), QK_FLOOR
    ).astype(jnp.bfloat16)
    value_heads = value_head.reshape(length, local_kv, head_dim)
    factor = (gain_local * head_dim ** (-0.5)).reshape(local_kv, group_size)
    out_gains = norm_local.reshape(local_kv, group_size, head_dim)
    key_totals = jnp.transpose(cumulative, (1, 2, 0))
    span_rows = 512
    positions = jnp.arange(length, dtype=jnp.int32)

    def attend_block(block_index):
        first = block_index * span_rows
        query_block = lax.dynamic_slice_in_dim(query_unit, first, span_rows, 0)
        query_totals = lax.dynamic_slice_in_dim(cumulative, first, span_rows, 0)
        scores = jnp.einsum(
            "qkgd,skd->kgqs", query_block, key_unit, preferred_element_type=jnp.float32
        )
        scores = (
            scores * factor[:, :, None, None]
            + jnp.transpose(query_totals, (1, 2, 0))[..., None]
            - key_totals[:, :, None, :]
        )
        allowed = positions[None, :] <= (first + jnp.arange(span_rows, dtype=jnp.int32))[:, None]
        scores = jnp.where(allowed[None, None], scores, NEG)
        row_peak = jnp.max(scores, axis=-1, keepdims=True)
        exponent = jnp.exp(scores - row_peak)
        weights = (exponent / jnp.sum(exponent, axis=-1, keepdims=True)).astype(jnp.bfloat16)
        mixed = jnp.einsum(
            "kgqs,skd->qkgd", weights, value_heads, preferred_element_type=jnp.float32
        )
        return (head_norm(mixed, OUT_FLOOR) * out_gains).astype(jnp.bfloat16)

    outputs = lax.map(attend_block, jnp.arange(length // span_rows, dtype=jnp.int32))
    outputs = outputs.reshape(length, local_heads, head_dim)
    back_rows = lax.all_to_all(outputs, "sp", split_axis=0, concat_axis=1, tiled=True)
    return back_rows.reshape(1, tok_count, head_count * head_dim)


def heads_on_dp(
    tokens,
    forget_offset,
    q_weight,
    k_weight,
    v_weight,
    forget_weight,
    forget_bias,
    score_gain,
    out_gain,
):
    tok_count = tokens.shape[1]
    head_count = forget_bias.shape[0]
    head_dim = out_gain.shape[0] // head_count
    seq_count = lax.axis_size("dp")
    kv = k_weight.shape[1] // head_dim
    heads = q_weight.shape[1] // head_dim
    group = heads // kv
    everyone = lax.all_gather(tokens, "dp", axis=0, tiled=True)
    offsets = lax.all_gather(forget_offset, "dp", axis=0, tiled=True)
    flat = everyone.reshape(seq_count * tok_count, -1)
    first = lax.axis_index("dp") * heads

    def mine(array):
        return lax.dynamic_slice_in_dim(array, first, heads, array.ndim - 1)

    def project(weight):
        return jnp.dot(flat, weight, preferred_element_type=jnp.float32).astype(jnp.bfloat16)

    key_unit = head_norm(
        project(k_weight).astype(jnp.float32).reshape(seq_count, tok_count, kv, head_dim), QK_FLOOR
    ).astype(jnp.bfloat16)
    values = project(v_weight).reshape(seq_count, tok_count, kv, head_dim)
    pair = lax.all_gather(jnp.stack([key_unit, values]), "sp", axis=2, tiled=True)
    forget_input = (
        jnp.dot(flat, mine(forget_weight), preferred_element_type=jnp.float32)
        + offsets.reshape(-1)[:, None]
    ).astype(jnp.bfloat16)
    log_gate = jax.nn.log_sigmoid(forget_input.astype(jnp.float32) + mine(forget_bias)[None, :])
    gates = lax.all_gather(
        log_gate.reshape(seq_count, tok_count, heads), "sp", axis=1, tiled=True
    )
    cumulative = jnp.cumsum(gates, axis=1)
    length = gates.shape[1]
    start = lax.axis_index("sp") * tok_count
    own = lax.dynamic_slice_in_dim(cumulative, start, tok_count, 1)
    query_unit = head_norm(
        project(q_weight).astype(jnp.float32).reshape(seq_count, tok_count, kv, group, head_dim),
        QK_FLOOR,
    ).astype(jnp.bfloat16)
    factor = (mine(score_gain) * head_dim ** (-0.5)).reshape(kv, group)
    scores = jnp.einsum(
        "bqkgd,bskd->bkgqs", query_unit, pair[0], preferred_element_type=jnp.float32
    )
    by_head = jnp.transpose(own.reshape(seq_count, tok_count, kv, group), (0, 2, 3, 1))
    by_key = jnp.transpose(cumulative.reshape(seq_count, length, kv, group), (0, 2, 3, 1))
    scores = (
        scores * factor[None, :, :, None, None] + by_head[..., None] - by_key[..., None, :]
    )
    allowed = jnp.arange(length)[None, :] <= (start + jnp.arange(tok_count))[:, None]
    scores = jnp.where(allowed, scores, NEG)
    exponent = jnp.exp(scores - jnp.max(scores, axis=-1, keepdims=True))
    weights = (exponent / jnp.sum(exponent, axis=-1, keepdims=True)).astype(jnp.bfloat16)
    mixed = jnp.einsum(
        "bkgqs,bskd->bqkgd", weights, pair[1], preferred_element_type=jnp.float32
    )
    gains = lax.dynamic_slice_in_dim(out_gain, first * head_dim, heads * head_dim, 0)
    outputs = (head_norm(mixed, OUT_FLOOR) * gains.reshape(kv, group, head_dim)).astype(
        jnp.bfloat16
    )
    outputs = outputs.reshape(seq_count, tok_count, heads * head_dim)
    return lax.all_to_all(outputs, "dp", split_axis=0, concat_axis=2, tiled=True)


LOG2E = 1.4426950408889634


def fused_kernel(
    tok_in,
    off_in,
    qw_in,
    kw_in,
    vw_in,
    fw_in,
    bias_in,
    gain_in,
    norm_in,
    result,
    tok,
    qw,
    kvw,
    fw,
    off,
    bias_row,
    gain,
    norm,
    q_unit,
    kv,
    running_all,
    gates,
    sent,
    load_sem,
    ready,
    off_send,
    off_recv,
    beside_send,
    beside_recv,
    over_send,
    cross_recv,
    onward_send,
    gate_send,
    gate_recv,
    kv_send,
    kv_recv,
    back_send,
    out_send,
    out_recv,
):
    d = lax.axis_index("dp")
    s = lax.axis_index("sp")
    spread = lax.axis_size("sp")
    rows, width = tok_in.shape
    half, quarter = rows // 2, rows // 4
    cols = qw_in.shape[1]
    head_dim = kw_in.shape[1]
    heads = cols // head_dim
    seqs = tok.shape[0]
    chip, core = d // 2, d % 2
    last = spread - 1
    scope = jax.named_scope

    def peer(step):
        across = step // 2
        own_chip = (1 - across) * ((core + step % 2) % 2)
        return ((chip + across) % 2) * 2 + across * (step % 2) + own_chip

    def seen_as(step):
        return (step // 2) * (2 + core) + (1 - step // 2) * step

    def remote(src, dst, send, recv, **target):
        return pltpu.make_async_remote_copy(
            src_ref=src,
            dst_ref=dst,
            send_sem=send,
            recv_sem=recv,
            device_id=target,
            device_id_type=pl.DeviceIdType.MESH,
        )

    barrier = pltpu.get_barrier_semaphore()
    for step in range(1, seqs):
        pl.semaphore_signal(
            barrier, inc=1, device_id={"dp": peer(step)}, device_id_type=pl.DeviceIdType.MESH
        )

    @pl.when(s > 0)
    def _():
        pl.semaphore_signal(
            barrier, inc=1, device_id={"sp": s - 1}, device_id_type=pl.DeviceIdType.MESH
        )

    @pl.when(s < last)
    def _():
        pl.semaphore_signal(
            barrier, inc=1, device_id={"sp": s + 1}, device_id_type=pl.DeviceIdType.MESH
        )

    def load(src, dst, index):
        copy = pltpu.make_async_copy(src, dst, load_sem.at[index])
        copy.start()
        return copy

    load_tok = load(tok_in, tok.at[0], 0)
    load_off = load(off_in, off.at[0], 1)
    load_k = load(kw_in, kvw.at[:, pl.ds(0, head_dim)], 2)
    load_v = load(vw_in, kvw.at[:, pl.ds(head_dim, head_dim)], 3)
    load_f = load(fw_in, fw, 4)
    load_b = load(bias_in, bias_row, 5)
    load_g = load(gain_in, gain, 6)
    load_n = load(norm_in, norm, 7)
    load_q = load(qw_in, qw, 8)

    load_tok.wait()
    load_off.wait()
    with scope("bar"):
        pl.semaphore_wait(barrier, seqs - 1 + (s + last) // spread + 1 - (s + 1) // spread)

    def tell_back(target):
        pl.semaphore_signal(
            ready.at[target], inc=1, device_id={"sp": s - 1}, device_id_type=pl.DeviceIdType.MESH
        )

    @pl.when(jnp.logical_and(s > 0, s < last))
    def _():
        tell_back(s + 1)

    def await_ready(source):
        for target in range(source + 2, spread):
            pl.semaphore_wait(ready.at[target], 1)
            if source > 0:
                tell_back(target)

    offs = [
        remote(off.at[0], off.at[seen_as(step)], off_send.at[0], off_recv.at[0], dp=peer(step))
        for step in range(1, seqs)
    ]
    for copy in offs:
        copy.start()

    def half_of(index):
        return pl.ds(pl.multiple_of(index * half, half), half)

    beside = [
        remote(
            tok.at[0, half_of(part)], tok.at[1, half_of(part)], beside_send.at[0],
            beside_recv.at[i], dp=peer(1),
        )
        for i, part in enumerate((1 - core, core))
    ]
    crossings = [
        (1, 3, 0, quarter),
        (0, 2, 0, half),
        (1, 2, half, half),
        (0, 3, quarter, quarter),
        (1, 3, half, quarter),
        (1, 3, half + quarter, quarter),
    ]
    over, onward = [], []
    for j, (sender, slot, first, count) in enumerate(crossings):
        part = pl.ds(first, count)
        held = 0 if sender == slot - 2 else 1
        over.append(
            remote(
                tok.at[held, part], tok.at[slot, part], over_send.at[0], cross_recv.at[j],
                dp=(1 - chip) * 2 + core,
            )
        )
        onward.append(
            remote(
                tok.at[slot, part], tok.at[slot, part], onward_send.at[0], cross_recv.at[j],
                dp=peer(1),
            )
        )

    @pl.when(core == 0)
    def _():
        over[1].start()

    @pl.when(core == 1)
    def _():
        over[0].start()

    for copy in beside:
        copy.start()

    def unit(vectors):
        vectors = vectors.astype(jnp.bfloat16).astype(jnp.float32)
        return head_norm(vectors, QK_FLOOR).astype(jnp.bfloat16)

    def returned(slot):
        return (last - 1, last - 1, 1, 1)[slot]

    def delayed(slot):
        return slot == 1

    def to_each(act):
        for target in range(last, 0, -1):

            @pl.when(s < target)
            def _():
                act(target)

    def halved(slot, block):
        return slot > 1 and block == 0

    def parts_of(slot, late):
        if slot < 2:
            return [(0, rows)]
        return [(pl.multiple_of((late + core - 2 * late * core) * half, half), half)]

    final = seqs - 1
    final_parts = {
        (0, 0): [(0, half + quarter)],
        (0, 1): [(half + quarter, quarter)],
        (1, 0): [(0, quarter), (half, quarter)],
        (1, 1): [(quarter, quarter), (half + quarter, quarter)],
    }

    def final_rows(c, late):
        return sum(count for _, count in final_parts[c, late])

    def on_core(act):
        for c in range(2):

            @pl.when(core == c)
            def _():
                act(c)

    def await_final(late):
        def act(c):
            group = kv_recv.at[final, last if late else 0]
            arrived(kv.at[final, :, pl.ds(0, final_rows(c, late))], group)

        on_core(act)

    def kv_copy(slot, first, count, target, late=False):
        piece = kv.at[slot, :, pl.ds(pl.multiple_of(s * rows + first, quarter), count)]
        group = s + late * (last - last * ((s + last) // spread))
        return remote(piece, piece, kv_send.at[target], kv_recv.at[slot, group], sp=target)

    def gate_copy(slot, target):
        piece = gates.at[slot, s]
        return remote(piece, piece, gate_send.at[target], gate_recv.at[slot], sp=target)

    def back_copy(slot, block, first, count, late):
        piece = kv.at[slot, :, pl.ds(block * rows + first, count)]
        group = last if late else block
        return remote(piece, piece, back_send.at[slot], kv_recv.at[slot, group], sp=last - 1)

    def send_kv(slot, *parts, late=False, straight=False):
        def act(target):
            skip_from = last - 1 if target == last and delayed(slot) else last
            for first, count in parts:
                skip_below = returned(slot) if target == last - 1 and not straight else 0

                @pl.when(jnp.logical_and(s >= skip_below, s < skip_from))
                def _():
                    kv_copy(slot, first, count, target, late).start()

        to_each(act)

    def send_gate(slot):
        to_each(lambda target: gate_copy(slot, target).start())

    def project_kv(slot, *parts):
        pair = jnp.dot(
            jnp.concatenate([tok[slot, first : first + count] for first, count in parts], axis=0),
            kvw[...],
            preferred_element_type=jnp.float32,
        )
        done = 0
        for first, count in parts:
            here = pl.ds(pl.multiple_of(s * rows + first, quarter), count)
            piece = pair[done : done + count]
            kv[slot, 0, here] = unit(piece[:, :head_dim])
            kv[slot, 1, here] = piece[:, head_dim:].astype(jnp.bfloat16)
            done += count

    def project_q(slot):
        queries = jnp.dot(tok[slot], qw[...], preferred_element_type=jnp.float32)
        for h in range(heads):
            q_unit[slot, pl.ds(h * rows, rows)] = unit(
                queries[:, h * head_dim : (h + 1) * head_dim]
            )

    count = bias_in.shape[1]

    def gate(slot):
        forget_input = (
            lax.dot_general(
                fw[...], tok[slot], (((1,), (1,)), ((), ())), preferred_element_type=jnp.float32
            )
            + off[slot]
        ).astype(jnp.bfloat16)
        square = (count, count)
        diagonal = lax.broadcasted_iota(jnp.int32, square, 0) == lax.broadcasted_iota(
            jnp.int32, square, 1
        )
        bias = jnp.sum(
            jnp.where(diagonal, jnp.broadcast_to(bias_row[...], square), 0.0),
            axis=1,
            keepdims=True,
        )
        gate_arg = forget_input.astype(jnp.float32) + bias
        log_gate = jnp.minimum(gate_arg, 0.0) - jnp.log1p(jnp.exp(-jnp.abs(gate_arg)))
        before = lax.broadcasted_iota(jnp.int32, (rows, rows), 0)
        after = lax.broadcasted_iota(jnp.int32, (rows, rows), 1)
        upto = (before <= after).astype(jnp.bfloat16)
        high = log_gate.astype(jnp.bfloat16)
        rest = log_gate - high.astype(jnp.float32)
        middle = rest.astype(jnp.bfloat16)
        low = (rest - middle.astype(jnp.float32)).astype(jnp.bfloat16)
        running = (
            jnp.dot(low, upto, preferred_element_type=jnp.float32)
            + jnp.dot(middle, upto, preferred_element_type=jnp.float32)
            + jnp.dot(high, upto, preferred_element_type=jnp.float32)
        )
        running_all[...] = running * LOG2E
        own = running_all[pl.ds(d * heads, heads)]
        spare = gates.shape[2] - heads
        if spare:
            own = jnp.concatenate([own, jnp.zeros((spare, rows), jnp.float32)], axis=0)
        gates[slot, s] = own

    def out_copy(slot, start, group):
        place = pl.ds(
            pl.multiple_of(d * cols + start * head_dim, head_dim), group * head_dim
        )
        return remote(
            sent.at[slot, :, pl.ds(start * head_dim, group * head_dim)], result.at[:, place],
            out_send.at[0], out_recv.at[0], dp=peer(slot),
        )

    def attend(slot, blocks, groups):
        span = blocks * rows
        later = jnp.zeros((gates.shape[2], 1), jnp.float32)
        totals = [gates[slot, blocks - 1]]
        for b in range(blocks - 2, -1, -1):
            local_sum = gates[slot, b]
            later = later + local_sum[:, rows - 1 :]
            totals.insert(0, local_sum - later)
        allowed = lax.broadcasted_iota(jnp.int32, (rows, rows), 1) <= lax.broadcasted_iota(
            jnp.int32, (rows, rows), 0
        )
        keys = kv[slot, 0, :span]
        values = kv[slot, 1, :span]
        start = 0
        for group in groups:
            each = range(start, start + group)
            raw = [
                lax.dot_general(
                    q_unit[slot, pl.ds(h * rows, rows)],
                    keys,
                    (((1,), (1,)), ((), ())),
                    preferred_element_type=jnp.float32,
                )
                for h in each
            ]
            scores = []
            for h, product in zip(each, raw):
                factor = gain[0, d * heads + h] * (head_dim ** (-0.5) * LOG2E)
                parts = [
                    product[:, b * rows : (b + 1) * rows] * factor - totals[b][h : h + 1, :]
                    for b in range(blocks)
                ]
                parts[-1] = jnp.where(allowed, parts[-1], NEG)
                scores.append(parts)
            peaks = [
                jnp.max(functools.reduce(jnp.maximum, parts), axis=-1, keepdims=True)
                for parts in scores
            ]
            exponents = [
                [jnp.exp2(part - peak) for part in parts] for parts, peak in zip(scores, peaks)
            ]
            scales = [
                1.0 / jnp.sum(functools.reduce(jnp.add, parts), axis=-1, keepdims=True)
                for parts in exponents
            ]
            weights = [
                jnp.concatenate([(part * scale).astype(jnp.bfloat16) for part in parts], axis=1)
                for parts, scale in zip(exponents, scales)
            ]
            mixed = [jnp.dot(w, values, preferred_element_type=jnp.float32) for w in weights]
            for h, rough in zip(each, mixed):
                place = pl.ds(pl.multiple_of(d * cols + h * head_dim, head_dim), head_dim)
                outcome = (head_norm(rough, OUT_FLOOR) * norm[:, place]).astype(jnp.bfloat16)
                if slot == 0:
                    result[:, place] = outcome
                else:
                    sent[slot, :, h * head_dim : (h + 1) * head_dim] = outcome
            if slot > 0:
                out_copy(slot, start, group).start()
            start += group

    in_turn = [1] * (heads // 2) + [heads - heads // 2]

    def arrived(ref, semaphore):
        pltpu.make_async_copy(ref, ref, semaphore).wait()

    def await_kv(slot, blocks):
        for b in blocks:
            if halved(slot, b) and slot == final:
                await_final(0)
                await_final(1)
            elif halved(slot, b):
                arrived(kv.at[slot, :, pl.ds(b * rows, half)], kv_recv.at[slot, b])
                arrived(kv.at[slot, :, pl.ds(b * rows, half)], kv_recv.at[slot, last])
            else:
                arrived(kv.at[slot, :, pl.ds(b * rows, rows)], kv_recv.at[slot, b])

    def send_back(slot, late=0):
        @pl.when(s == last)
        def _():
            with scope(f"bk{slot}{late}"):
                if slot == final:
                    await_final(late)
                elif slot > 1:
                    group = kv_recv.at[slot, last if late else 0]
                    arrived(kv.at[slot, :, pl.ds(0, half)], group)
                else:
                    await_kv(slot, range(returned(slot)))
            if slot == final:

                def act(c):
                    if (c, late) != (0, 1):
                        for first, count in final_parts[c, late]:
                            back_copy(slot, 0, first, count, late).start()

                on_core(act)
            else:
                for b in range(returned(slot)):
                    for first, count in parts_of(slot, late):
                        back_copy(slot, b, first, count, late).start()

    def attend_at(slot, places):
        for k in places:

            @pl.when(s == k)
            def _():
                if k > 0:
                    with scope(f"wkv{slot}"):
                        arrived(gates.at[slot, pl.ds(0, k)], gate_recv.at[slot])
                        await_kv(slot, range(returned(slot) if k == last else 0, k))
                with scope(f"att{slot}"):
                    attend(slot, k + 1, in_turn if slot == seqs - 1 else [heads])

    def direct(j):
        with scope(f"wx{j}"):
            over[j].wait_recv()
        onward[j].start()

    def passed(j):
        with scope(f"wo{j}"):
            onward[j].wait_recv()

    def whole(j):
        return crossings[j][2:]

    def treat(slot, *js, ends=False, late=False, straight=False):
        parts = [whole(j) for j in js]
        with scope(f"p{slot}" + "".join(map(str, js))):
            project_kv(slot, *parts)
            if ends:
                gate(slot)
        if ends:
            send_gate(slot)
        send_kv(slot, *parts, late=late, straight=straight)

    load_k.wait()
    load_v.wait()
    with scope("pkv0"):
        project_kv(0, (0, rows))
    for source in range(1, spread - 1):

        @pl.when(s == source)
        def _():
            await_ready(source)

    @pl.when(s > 0)
    def _():
        send_kv(0, (0, rows))

    with scope("wb0"):
        beside[0].wait_recv()

    @pl.when(core == 0)
    def _():
        over[3].start()

    @pl.when(core == 1)
    def _():
        over[2].start()
        over[4].start()
        over[5].start()

    load_f.wait()
    load_b.wait()
    with scope("wb1"):
        beside[1].wait_recv()
    with scope("pkv1g0"):
        gate(0)
        project_kv(1, (0, rows))

    @pl.when(s == 0)
    def _():
        with scope("rdy"):
            await_ready(0)
        send_kv(0, (0, rows))

    send_gate(0)
    send_kv(1, (0, rows))
    load_q.wait()
    load_g.wait()
    load_n.wait()
    with scope("woff"):
        arrived(off.at[pl.ds(1, seqs - 1)], off_recv.at[0])
    with scope("pq01g1"):
        gate(1)
        project_q(0)
        project_q(1)
    send_gate(1)

    @pl.when(core == 0)
    def _():
        passed(0)
        treat(3, 0)
        send_back(0)
        direct(1)
        treat(2, 1)
        send_back(1)
        passed(2)
        treat(2, 2, ends=True, late=True)

    @pl.when(core == 1)
    def _():
        direct(0)
        treat(3, 0)
        send_back(0)
        direct(2)
        treat(2, 2)
        send_back(1)
        passed(1)
        treat(2, 1, ends=True, late=True)

    with scope("pq2"):
        project_q(2)
    send_back(2)
    attend_at(0, [last])

    @pl.when(core == 0)
    def _():
        direct(3)
        treat(3, 3)
        passed(4)
        treat(3, 4)
        send_back(2, 1)
        passed(5)
        treat(3, 5, ends=True, late=True, straight=True)

    @pl.when(core == 1)
    def _():
        direct(4)
        treat(3, 4)
        direct(5)
        treat(3, 5, late=True)
        send_back(2, 1)
        passed(3)
        treat(3, 3, ends=True, late=True)

    for slot in range(seqs):
        if delayed(slot):

            @pl.when(s == last - 1)
            def _():
                kv_copy(slot, 0, rows, last).start()

    with scope("pq3"):
        project_q(3)
    attend_at(2, [0])
    attend_at(3, [0])
    attend_at(0, [last - 1])
    attend_at(1, [last - 1])
    send_back(3)
    send_back(3, 1)
    attend_at(2, [last])
    attend_at(2, range(1, last))
    attend_at(0, range(last - 1))
    attend_at(1, range(last - 1))
    attend_at(3, range(1, spread))
    attend_at(1, [last])

    with scope("flush"):
        arrived(sent.at[pl.ds(1, seqs - 1)], out_recv.at[0])
    with scope("drain"):
        arrived(sent.at[pl.ds(1, seqs - 1)], out_send.at[0])
        arrived(off.at[pl.ds(1, seqs - 1)], off_send.at[0])
        arrived(tok.at[0], beside_send.at[0])
        for sender in range(2):
            many = sum(item[3] for item in crossings if item[0] == sender)

            @pl.when(core == sender)
            def _():
                for semaphore in (over_send, onward_send):
                    arrived(tok.at[pl.ds(0, 2), pl.ds(0, many // 2)], semaphore.at[0])

        def sent_to(target):
            arrived(gates.at[pl.ds(0, seqs), 0], gate_send.at[target])
            for source in range(target):
                skipped = sum(
                    target == last - 1 and source < returned(slot) for slot in range(seqs)
                )
                if skipped == seqs:

                    @pl.when(jnp.logical_and(s == source, core == 0))
                    def _():
                        arrived(
                            kv.at[final, :, pl.ds(0, final_rows(0, 1))], kv_send.at[target]
                        )

                    continue

                @pl.when(s == source)
                def _():
                    arrived(
                        kv.at[pl.ds(skipped, seqs - skipped), :, pl.ds(0, rows)],
                        kv_send.at[target],
                    )

        to_each(sent_to)

        @pl.when(s == last)
        def _():
            for slot in range(seqs):
                if slot < final:
                    arrived(kv.at[slot, :, pl.ds(0, returned(slot) * rows)], back_send.at[slot])

            def act(c):
                many = rows if c else final_rows(0, 0)
                arrived(kv.at[final, :, pl.ds(0, many)], back_send.at[final])

            on_core(act)


def fused(
    tokens,
    forget_offset,
    q_weight,
    k_weight,
    v_weight,
    forget_weight,
    forget_bias,
    score_gain,
    out_gain,
):
    rows, width = tokens.shape[1:]
    head_count = forget_bias.shape[0]
    head_dim = out_gain.shape[0] // head_count
    seqs = lax.axis_size("dp")
    spread = lax.axis_size("sp")
    cols = q_weight.shape[1]
    heads = cols // head_dim
    padded = -(-heads // 8) * 8
    outside = pl.BlockSpec(memory_space=pltpu.HBM)
    dma = pltpu.SemaphoreType.DMA
    out = pl.pallas_call(
        fused_kernel,
        out_shape=pltpu.VMEM((rows, seqs * cols), jnp.bfloat16),
        in_specs=[outside] * 9,
        out_specs=pl.BlockSpec(memory_space=pltpu.VMEM),
        scratch_shapes=[
            pltpu.VMEM((seqs, rows, width), jnp.bfloat16),
            pltpu.VMEM((width, cols), jnp.bfloat16),
            pltpu.VMEM((width, 2 * head_dim), jnp.bfloat16),
            pltpu.VMEM((head_count, width), jnp.bfloat16),
            pltpu.VMEM((seqs, 1, rows), jnp.float32),
            pltpu.VMEM((1, head_count), jnp.float32),
            pltpu.SMEM((1, head_count), jnp.float32),
            pltpu.VMEM((1, head_count * head_dim), jnp.float32),
            pltpu.VMEM((seqs, heads * rows, head_dim), jnp.bfloat16),
            pltpu.VMEM((seqs, 2, spread * rows, head_dim), jnp.bfloat16),
            pltpu.VMEM((head_count, rows), jnp.float32),
            pltpu.VMEM((seqs, spread, padded, rows), jnp.float32),
            pltpu.VMEM((seqs, rows, cols), jnp.bfloat16),
            dma((9,)),
            pltpu.SemaphoreType.REGULAR((spread,)),
            dma((1,)),
            dma((1,)),
            dma((1,)),
            dma((2,)),
            dma((1,)),
            dma((6,)),
            dma((1,)),
            dma((spread,)),
            dma((seqs,)),
            dma((spread,)),
            dma((seqs, spread)),
            dma((seqs,)),
            dma((1,)),
            dma((1,)),
        ],
        compiler_params=pltpu.CompilerParams(
            collective_id=0, has_side_effects=True
        ),
    )(
        tokens[0],
        forget_offset,
        q_weight,
        k_weight,
        v_weight,
        forget_weight.T,
        forget_bias[None, :],
        score_gain[None, :],
        out_gain[None, :],
    )
    return out[None]


def local(*args):
    tokens, k_weight, forget_bias, out_gain = args[0], args[3], args[6], args[8]
    head_dim = out_gain.shape[0] // forget_bias.shape[0]
    fits = tokens.shape[0] == 1 and tokens.shape[1] % 128 == 0 and head_dim % 128 == 0
    if (
        lax.axis_size("dp") == 4
        and 2 < lax.axis_size("sp") <= 4
        and k_weight.shape[1] == head_dim
        and fits
    ):
        return fused(*args)
    if k_weight.shape[1] % head_dim == 0 and tokens.shape[0] == 1:
        return heads_on_dp(*args)
    return heads_on_sp(*args)


def solution(mesh):
    in_specs = (
        P(("grp", "dp"), "sp", None),
        P(("grp", "dp"), "sp"),
        P(None, "dp"),
        P(None, "dp"),
        P(None, "dp"),
        P(),
        P(),
        P(),
        P(),
    )
    out_specs = P(("grp", "dp"), "sp", None)
    return jax.shard_map(local, mesh=mesh, in_specs=in_specs, out_specs=out_specs, check_vma=False)
```
